768 devices in a mesh: ep: 24 (over z, core), tp: 32 (over y, x).
Axes of the slice: x: 4, y: 8, z: 12, core: 2. Of those that a mesh axis runs over, the one named last changes fastest.
Arguments:
- tokens: bfloat16 [98304, 2048], P(('ep', 'tp')), may hold values from -40 to 40
- norm_gain: float32 [2048], replicated, may hold values from 0.1 to 1.9
- routes: int32 [98304, 2], P(('ep', 'tp')), may hold values from 0 to 31, all different within a row; in each aligned block of 128 rows (0 to 127, 128 to 255, ...) at most 16 rows name the same one
- gates: float32 [98304, 2], P(('ep', 'tp')), may hold values from 0.25 to 2
- expert_gate: bfloat16 [32, 2048, 512], P('tp'), may hold values from -0.125 to 0.125
- expert_up: bfloat16 [32, 2048, 512], P('tp'), may hold values from -0.125 to 0.125
- expert_down: bfloat16 [32, 512, 2048], P('tp'), may hold values from -0.25 to 0.25
- shared_gate: bfloat16 [2048, 256], replicated, may hold values from -0.125 to 0.125
- shared_up: bfloat16 [2048, 256], replicated, may hold values from -0.125 to 0.125
- shared_down: bfloat16 [256, 2048], replicated, may hold values from -0.375 to 0.375
Outputs:
- mixed: bfloat16 [98304, 2048], P(('ep', 'tp'))
- load: float32 [32], replicated
The draws below stay inside these ranges and needn't reach their ends.
Inputs may be any that keep to these rules, and one draw needn't show every extreme that they name: `routes`: each row names 2 different experts. Among the rows of one device no expert is named by more than 16 rows, and in every draw some expert is named by exactly 16 rows of some device.
All inputs are finite; a program needn't handle non-finite values.
Results may differ from the reference program's by a relative error of at most 0.002.
The reference program's roundings to bfloat16 on the way count: a program that leaves them out, or rounds other values in their place, can miss the bound.
Values may be sent and summed in bfloat16 or wider, within the bound.
A program may use at most 64 MiB of HBM per device.

```python
import math
import jax
import jax.numpy as jnp
import numpy as np
from jax import lax

D = 2048
EXPERT_UNITS = 512
SHARED = 256
TOPK = 2
TOK_DEV = 128
EXPERTS = 32
CAP = 16
TOKENS = 98304


def draw_tokens(key, part):
    key_values, key_column, key_row = jax.random.split(key, 3)
    column_scale = jnp.exp(jax.random.uniform(key_column, (D,), jnp.float32, jnp.log(0.5), jnp.log(5.0)))
    row_scale = jnp.exp(jax.random.uniform(key_row, (TOKENS, 1), jnp.float32, jnp.log(0.5), jnp.log(2.0)))
    base_values = jnp.clip(jax.random.normal(key_values, (TOKENS, D), jnp.float32), -4.0, 4.0)
    return (base_values * column_scale * row_scale).astype(jnp.bfloat16)


def level_of(stream_key, shape, pieces, low, high):
    level, own = 1.0, jax.random.fold_in(stream_key, 6)
    for axis_at, parts in pieces:
        heights = jnp.exp(jax.random.uniform(jax.random.fold_in(own, axis_at), (parts,), jnp.float32, low / len(pieces), high / len(pieces)))
        level = level * jnp.repeat(heights, shape[axis_at] // parts).reshape([-1 if axis == axis_at else 1 for axis in range(len(shape))])
    return level


def routed_block(own_key, own, number, rows, number_of, top, bound, skew):
    ranking = jax.random.permutation(own_key, number_of)
    crowded, ordinary = load_shares(number_of, rows * top, bound, skew, True), load_shares(number_of, rows * top, bound, skew, False)
    places = jnp.arange(number_of)

    def named(lengths, rotation):
        used = int((lengths > 0).sum())
        fixed = max(1, used // 4)
        passed = fixed + (places - fixed + rotation * (used - fixed)) % max(1, number_of - fixed)
        return jnp.zeros((number_of,), jnp.int32).at[ranking[jnp.where(places < fixed, places, passed)]].set(jnp.asarray(lengths, jnp.int32))

    lengths = jnp.where(number % 4 == 0, named(crowded, number // 4), named(ordinary, number - number // 4 - 1))
    mixed = jax.random.permutation(jax.random.fold_in(own, 3), number_of)
    donor, sink = mixed[0:number_of // 2 * 2:2], mixed[1:number_of // 2 * 2:2]
    slack = jnp.minimum(lengths[donor] - 1, bound - lengths[sink]) // 2
    slack = jnp.where((donor == ranking[0]) | (sink == ranking[0]) | (lengths[sink] == 0), 0, jnp.maximum(slack, 0))
    passed = jax.random.randint(jax.random.fold_in(own, 4), (number_of // 2,), 0, 1 << 20) % (slack + 1)
    lengths = lengths.at[donor].add(-passed).at[sink].add(passed)
    items = jnp.searchsorted(jnp.cumsum(lengths), jnp.arange(rows * top), side="right").astype(jnp.int32)
    table = items.reshape(top, rows).T
    table = table[jax.random.permutation(jax.random.fold_in(own, 1), rows)]
    rotation = jax.random.randint(jax.random.fold_in(own, 2), (rows, 1), 0, top)
    return jnp.take_along_axis(table, (jnp.arange(top)[None, :] + rotation) % top, axis=1)


def load_shares(amount, total, reach, lean, full):
    portions = [(1 << 20) // math.isqrt(grade ** lean) + 1 for grade in range(1, amount + 1)]
    largest = reach if full else min(reach, max(-(-total // amount), total * portions[0] // sum(portions)))
    least = 1 if total - largest >= amount - 1 else 0
    given, rest = [largest] + [least] * (amount - 1), total - largest - least * (amount - 1)
    while rest > 0:
        candidates = [i for i in range(1, amount) if given[i] < largest] or [i for i in range(1, amount) if given[i] < reach]
        whole, budget = sum([portions[i] for i in candidates]), rest
        for i in candidates:
            more = min(reach - given[i], max(1, budget * portions[i] // whole), rest)
            given[i] = given[i] + more
            rest = rest - more
    return np.array(given)


def scatter_about(key, extent, deviation, reach, cuts=(), kind=jnp.bfloat16):
    gain = level_of(key, extent, cuts, -0.22, 0.18) if cuts else 1.0
    drawn = jax.random.normal(key, extent, jnp.float32) * deviation * gain
    return jnp.minimum(jnp.maximum(drawn, -reach), reach).astype(kind)


def setup_inputs(seed: int = 0) -> dict:
    streams_of = jax.random.split(jax.random.key(seed), 11)
    tokens = draw_tokens(jax.random.fold_in(streams_of[10], 71), 0)
    norm_gain = jnp.clip(1.0 + 0.18 * jax.random.normal(streams_of[1], (D,), jnp.float32), 0.1, 1.9)
    routes_keys = jax.random.split(jax.random.fold_in(streams_of[2], 1), TOKENS // TOK_DEV)
    routes_turns = jax.random.permutation(jax.random.fold_in(streams_of[2], 3), TOKENS // TOK_DEV)
    routes = jax.vmap(lambda own, number: routed_block(jax.random.fold_in(streams_of[2], 2), own, number, TOK_DEV, EXPERTS, TOPK, CAP, 2))(routes_keys, routes_turns).reshape((TOKENS, TOPK))
    gates = jnp.clip(0.25 + 1.75 * jax.random.uniform(streams_of[3], (TOKENS, TOPK), jnp.float32) ** level_of(streams_of[3], (TOKENS, TOPK), ((0, 768),), -0.2, 0.2), 0.25, 2.0)
    expert_gate = scatter_about(streams_of[4], (EXPERTS, D, EXPERT_UNITS), D ** -0.5, 0.125, ((0, 32),))
    expert_up = scatter_about(streams_of[5], (EXPERTS, D, EXPERT_UNITS), D ** -0.5, 0.125, ((0, 32),))
    expert_down = scatter_about(streams_of[6], (EXPERTS, EXPERT_UNITS, D), EXPERT_UNITS ** -0.5, 0.25, ((0, 32),))
    shared_gate = scatter_about(streams_of[7], (D, SHARED), D ** -0.5, 0.125)
    shared_up = scatter_about(streams_of[8], (D, SHARED), D ** -0.5, 0.125)
    shared_down = scatter_about(streams_of[9], (SHARED, D), SHARED ** -0.5, 0.375)
    return dict(tokens=tokens, norm_gain=norm_gain, routes=routes, gates=gates, expert_gate=expert_gate, expert_up=expert_up, expert_down=expert_down, shared_gate=shared_gate, shared_up=shared_up, shared_down=shared_down)


block_rows = 512

def layer_normed(token_block, norm_gain):
    values = token_block.astype(jnp.float32)
    center = lax.optimization_barrier(jnp.mean(values, axis=-1, keepdims=True))
    spread = lax.optimization_barrier(jnp.mean(jnp.square(values - center), axis=-1, keepdims=True))
    return ((values - center) * lax.rsqrt(spread + 1e-05) * norm_gain).astype(jnp.bfloat16)

def gated_mlp(row_block, w_gate, w_up, w_down):
    gate_part = jnp.dot(row_block, w_gate, preferred_element_type=jnp.float32)
    up_part = jnp.dot(row_block, w_up, preferred_element_type=jnp.float32)
    hidden = (jax.nn.silu(gate_part) * up_part).astype(jnp.bfloat16)
    return jnp.dot(hidden, w_down, preferred_element_type=jnp.float32)

def reference(tokens, norm_gain, routes, gates, expert_gate, expert_up, expert_down, shared_gate, shared_up, shared_down):
    normed = layer_normed(tokens, norm_gain)
    count_rows, feature_count = normed.shape
    copy_count = count_rows * TOPK
    flat_expert = routes.reshape(-1).astype(jnp.int32)
    flat_token = jnp.repeat(jnp.arange(count_rows, dtype=jnp.int32), TOPK)
    sort_order = jnp.argsort(flat_expert, stable=True).astype(jnp.int32)
    sorted_expert = flat_expert[sort_order]
    counts = lax.optimization_barrier(jnp.sum((flat_expert[:, None] == jnp.arange(EXPERTS, dtype=jnp.int32)[None, :]).astype(jnp.int32), axis=0))
    padded = (counts + block_rows - 1) // block_rows * block_rows
    starts = jnp.cumsum(counts) - counts
    block_ends = jnp.cumsum(padded)
    padded_starts = block_ends - padded
    destination = (padded_starts[sorted_expert] + jnp.arange(copy_count, dtype=jnp.int32) - starts[sorted_expert]).astype(jnp.int32)
    block_count = -(-copy_count // block_rows) + EXPERTS
    slot_token = jnp.full((block_count * block_rows,), count_rows, jnp.int32).at[destination].set(flat_token[sort_order])
    block_expert = jnp.clip(jnp.searchsorted(block_ends, jnp.arange(block_count, dtype=jnp.int32) * block_rows, side='right'), 0, EXPERTS - 1).astype(jnp.int32)
    padded_rows = jnp.concatenate([normed, jnp.zeros((1, feature_count), normed.dtype)], axis=0)

    def run_block(block_item):
        slot_tokens, expert = block_item
        row_block = padded_rows[slot_tokens]
        return gated_mlp(row_block, expert_gate[expert], expert_up[expert], expert_down[expert]).astype(jnp.bfloat16)
    slot_out = lax.map(run_block, (slot_token.reshape(block_count, block_rows), block_expert))
    slot_out = slot_out.reshape(block_count * block_rows, feature_count)
    copy_slot = jnp.zeros((copy_count,), jnp.int32).at[sort_order].set(destination).reshape(count_rows, TOPK)
    routed = jnp.zeros((count_rows, feature_count), jnp.float32)
    for choice_index in range(TOPK):
        picked = slot_out[copy_slot[:, choice_index]].astype(jnp.float32)
        routed = routed + gates[:, choice_index][:, None] * picked
    shared_out = gated_mlp(normed, shared_gate, shared_up, shared_down)
    mixed = (routed + shared_out).astype(jnp.bfloat16)
    load = counts.astype(jnp.float32) * (EXPERTS / (count_rows * TOPK))
    return (mixed, load)
```

```python
import functools

import jax
import jax.numpy as jnp
from jax import lax
from jax.experimental import pallas as pl
from jax.experimental.pallas import tpu as pltpu
from jax.sharding import PartitionSpec as P

NY, NX, NZ = 8, 4, 12
CAP = 16
MESH = pl.DeviceIdType.MESH
F32, BF16 = jnp.float32, jnp.bfloat16

SLOTS = [(dy, dx) for dx in (0, 1, 3, 2) for dy in (0, 4, 3, 5, 2, 6, 1, 7)]
GROUP = 8
ROWS = GROUP * CAP
GROUPS = len(SLOTS) // GROUP


def kernel(
    routes_ref,
    gates_ref,
    gain_ref,
    tokens_hbm,
    wg_hbm,
    wu_hbm,
    wd_hbm,
    sg_hbm,
    su_hbm,
    sd_hbm,
    mixed_ref,
    load_ref,
    tok,
    normed,
    wg,
    wu,
    wd,
    sg,
    su,
    sd,
    outgoing,
    arrived,
    result,
    returned,
    hidden,
    shidden,
    acc,
    csrc,
    cdst,
    local_sem,
    send_sem,
    recv_sem,
    back_send,
    back_recv,
    csend,
    crecv,
):
    ep, tp = lax.axis_index("ep"), lax.axis_index("tp")
    my_y, my_x = tp // NX, tp % NX
    my_z, my_c = ep // 2, ep % 2

    def plane(dy, dx):
        return {"tp": ((my_y + dy) % NY) * NX + (my_x + dx) % NX}

    def along_z(dz):
        return {"ep": ((my_z + dz) % NZ) * 2 + my_c}

    partner = {"ep": my_z * 2 + 1 - my_c}

    copies = [
        pltpu.make_async_copy(src, dst, local_sem.at[i])
        for i, (src, dst) in enumerate(
            [
                (tokens_hbm, tok),
                (sg_hbm, sg),
                (su_hbm, su),
                (sd_hbm, sd),
                (wg_hbm.at[0], wg),
                (wu_hbm.at[0], wu),
                (wd_hbm.at[0], wd),
            ]
        )
    ]
    for c in copies:
        c.start()

    peers = (
        [plane(dy, dx) for dy, dx in SLOTS if (dy, dx) != (0, 0)]
        + [along_z(dz) for dz in range(1, NZ)]
        + [partner]
    )
    barrier = pltpu.get_barrier_semaphore()
    for peer in peers:
        pl.semaphore_signal(barrier, inc=1, device_id=peer, device_id_type=MESH)

    routes = routes_ref[...]
    lane = lax.broadcasted_iota(jnp.int32, (1, 128), 1)
    lane_expert = jnp.full((1, 128), -1, jnp.int32)
    for j, (dy, dx) in enumerate(SLOTS):
        expert = ((my_y + dy) % NY) * NX + (my_x + dx) % NX
        lane_expert = jnp.where(lane == j, expert, lane_expert)
    ti = lax.broadcasted_iota(jnp.int32, (128, 128), 0)
    tj = lax.broadcasted_iota(jnp.int32, (128, 128), 1)
    hot = [(routes[:, k : k + 1] == lane_expert).astype(F32) for k in range(2)]
    both = (hot[0] + hot[1]).astype(BF16)
    earlier = jnp.dot((tj < ti).astype(F32).astype(BF16), both, preferred_element_type=F32)
    at = earlier + (CAP * lane).astype(F32)
    pos = [jnp.sum(h * at, axis=1, keepdims=True).astype(jnp.int32) for h in hot]
    pos_row = [
        jnp.sum(jnp.where(ti == tj, p, 0), axis=0, keepdims=True) for p in pos
    ]
    absolute = [(routes[:, k : k + 1] == lane).astype(F32) for k in range(2)]
    counts = jnp.sum(absolute[0] + absolute[1], axis=0, keepdims=True)
    csrc[0] = jnp.broadcast_to(counts, (8, 128))

    copies[0].wait()
    gain = gain_ref[...]

    def norm(i, carry):
        rows = pl.ds(pl.multiple_of(i * 16, 16), 16)
        values = tok[rows, :].astype(F32)
        values = values - jnp.mean(values, axis=-1, keepdims=True)
        spread = jnp.mean(values * values, axis=-1, keepdims=True)
        normed[rows, :] = (values * lax.rsqrt(spread + 1e-05) * gain).astype(BF16)
        return carry

    lax.fori_loop(0, 8, norm, 0)

    def build(g):
        rows = slice(g * ROWS, (g + 1) * ROWS)
        pick = jnp.where((ti + g * ROWS == pos_row[0]) | (ti + g * ROWS == pos_row[1]), 1.0, 0.0)
        pick = pick.astype(BF16)
        for n in range(4):
            cols = slice(n * 512, (n + 1) * 512)
            outgoing[rows, cols] = jnp.dot(
                pick, normed[:, cols], preferred_element_type=F32
            ).astype(BF16)

    def dispatch(j):
        rows = pl.ds(j * CAP, CAP)
        return pltpu.make_async_remote_copy(
            src_ref=outgoing.at[rows],
            dst_ref=arrived.at[rows],
            send_sem=send_sem.at[j],
            recv_sem=recv_sem.at[j],
            device_id=plane(*SLOTS[j]),
            device_id_type=MESH,
        )

    def give_back(j):
        rows = pl.ds(j * CAP, CAP)
        dy, dx = SLOTS[j]
        return pltpu.make_async_remote_copy(
            src_ref=result.at[rows],
            dst_ref=returned.at[rows],
            send_sem=back_send.at[j],
            recv_sem=back_recv.at[j],
            device_id=plane(-dy, -dx),
            device_id_type=MESH,
        )

    def in_group(g):
        return [j for j in range(g * GROUP, (g + 1) * GROUP) if j != 0]

    stages = (
        [plane(0, d) for d in range(1, NX)],
        [plane(d, 0) for d in range(1, NY)],
        [along_z(d) for d in range(1, NZ)],
        [partner],
    )
    starts = [sum(len(s) for s in stages[:i]) for i in range(len(stages))]

    def count_copy(stage, i):
        n = starts[stage] + i
        return pltpu.make_async_remote_copy(
            src_ref=csrc.at[stage],
            dst_ref=cdst.at[n],
            send_sem=csend.at[n],
            recv_sem=crecv.at[n],
            device_id=stages[stage][i],
            device_id_type=MESH,
        )

    def count_send(stage):
        for i in range(len(stages[stage])):
            count_copy(stage, i).start()

    def count_sum(stage):
        total = csrc[stage]
        for i in range(len(stages[stage])):
            count_copy(stage, i).wait_recv()
            total = total + cdst[starts[stage] + i]
        return total

    build(0)
    arrived[0:CAP, :] = outgoing[0:CAP, :]
    pl.semaphore_wait(barrier, len(peers))
    for g in range(GROUPS):
        if g + 1 < GROUPS:
            build(g + 1)
        for j in in_group(g):
            dispatch(j).start()
    count_send(0)

    for c in copies[1:4]:
        c.wait()
    gate = jnp.dot(normed[...], sg[...], preferred_element_type=F32)
    up = jnp.dot(normed[...], su[...], preferred_element_type=F32)
    shidden[...] = (gate / (1.0 + jnp.exp(-gate)) * up).astype(BF16)
    for n in range(4):
        cols = slice(n * 512, (n + 1) * 512)
        acc[:, cols] = jnp.dot(shidden[...], sd[:, cols], preferred_element_type=F32)

    csrc[1] = count_sum(0)
    count_send(1)

    for c in copies[4:]:
        c.wait()
    for g in range(GROUPS):
        rows = slice(g * ROWS, (g + 1) * ROWS)
        for j in in_group(g):
            dispatch(j).wait_recv()
        for n in range(2):
            cols = slice(n * 256, (n + 1) * 256)
            gate = jnp.dot(arrived[rows, :], wg[:, cols], preferred_element_type=F32)
            up = jnp.dot(arrived[rows, :], wu[:, cols], preferred_element_type=F32)
            hidden[:, cols] = (gate / (1.0 + jnp.exp(-gate)) * up).astype(BF16)
        for n in range(4):
            cols = slice(n * 512, (n + 1) * 512)
            result[rows, cols] = jnp.dot(
                hidden[...], wd[:, cols], preferred_element_type=F32
            ).astype(BF16)
        if g == 0:
            returned[0:CAP, :] = result[0:CAP, :]
        for j in in_group(g):
            give_back(j).start()
        if g == 1:
            csrc[2] = count_sum(1)
            count_send(2)
        if g == 3:
            csrc[3] = count_sum(2)
            count_send(3)

    weight = [gates_ref[:, k : k + 1] for k in range(2)]
    for g in range(GROUPS):
        rows = slice(g * ROWS, (g + 1) * ROWS)
        pick = jnp.concatenate(
            [jnp.where(tj + g * ROWS == p, 1.0, 0.0).astype(BF16) for p in pos], axis=0
        )
        for j in in_group(g):
            give_back(j).wait_recv()
        for n in range(4):
            cols = slice(n * 512, (n + 1) * 512)
            pair = jnp.dot(pick, returned[rows, cols], preferred_element_type=F32)
            total = acc[:, cols] + (weight[0] * pair[:128] + weight[1] * pair[128:])
            if g + 1 < GROUPS:
                acc[:, cols] = total
            else:
                mixed_ref[:, cols] = total.astype(BF16)

    load_ref[...] = count_sum(3) * (32 / 196608)
    for j in range(1, len(SLOTS)):
        dispatch(j).wait_send()
        give_back(j).wait_send()
    for stage in range(4):
        for i in range(len(stages[stage])):
            count_copy(stage, i).wait_send()


def per_device(tokens, norm_gain, routes, gates, wg, wu, wd, sg, su, sd):
    vmem = pl.BlockSpec(memory_space=pltpu.VMEM)
    anywhere = pl.BlockSpec(memory_space=pl.ANY)
    dma = pltpu.SemaphoreType.DMA
    slots = len(SLOTS)
    total = slots * CAP
    ncount = NX - 1 + NY - 1 + NZ - 1 + 1
    mixed, load = pl.pallas_call(
        kernel,
        out_shape=(
            jax.ShapeDtypeStruct((128, 2048), BF16),
            jax.ShapeDtypeStruct((8, 128), F32),
        ),
        in_specs=[vmem] * 3 + [anywhere] * 7,
        out_specs=(vmem, vmem),
        scratch_shapes=[
            pltpu.VMEM((128, 2048), BF16),
            pltpu.VMEM((128, 2048), BF16),
            pltpu.VMEM((2048, 512), BF16),
            pltpu.VMEM((2048, 512), BF16),
            pltpu.VMEM((512, 2048), BF16),
            pltpu.VMEM((2048, 256), BF16),
            pltpu.VMEM((2048, 256), BF16),
            pltpu.VMEM((256, 2048), BF16),
            pltpu.VMEM((total, 2048), BF16),
            pltpu.VMEM((total, 2048), BF16),
            pltpu.VMEM((total, 2048), BF16),
            pltpu.VMEM((total, 2048), BF16),
            pltpu.VMEM((ROWS, 512), BF16),
            pltpu.VMEM((128, 256), BF16),
            pltpu.VMEM((128, 2048), F32),
            pltpu.VMEM((4, 8, 128), F32),
            pltpu.VMEM((ncount, 8, 128), F32),
            dma((7,)),
            dma((slots,)),
            dma((slots,)),
            dma((slots,)),
            dma((slots,)),
            dma((ncount,)),
            dma((ncount,)),
        ],
        compiler_params=pltpu.CompilerParams(
            collective_id=0, has_side_effects=True, vmem_limit_bytes=56 << 20
        ),
    )(routes, gates, norm_gain.reshape(1, -1), tokens, wg, wu, wd, sg, su, sd)
    return mixed, load[0, :32]


def solution(mesh):
    rows = P(("ep", "tp"), None)
    expert = P("tp", None, None)
    return jax.shard_map(
        per_device,
        mesh=mesh,
        in_specs=(rows, P(), rows, rows, expert, expert, expert, P(), P(), P()),
        out_specs=(rows, P()),
        check_vma=False,
    )
```

```python
import jax
import jax.numpy as jnp
from jax import lax
from jax.experimental import pallas as pl
from jax.experimental.pallas import tpu as pltpu
from jax.sharding import PartitionSpec as P

NY, NX, NZ = 8, 4, 12
CAP = 16
MESH = pl.DeviceIdType.MESH
F32, BF16 = jnp.float32, jnp.bfloat16

SHIFTS = (-2, 2, -1, 1, 0)
FIRST_B = 2
TO_A = len(SHIFTS) * NX
SLOTS = TO_A + (len(SHIFTS) - FIRST_B) * NX
GROUP = 2 * NX
ROWS = GROUP * CAP
SELF_A, SELF_B = TO_A - NX, SLOTS - NX
SUBS = 4
SUB = 512 // SUBS


def kernel(
    routes_ref,
    gates_ref,
    gain_ref,
    tokens_hbm,
    wg_hbm,
    wu_hbm,
    wd_hbm,
    sg_hbm,
    su_hbm,
    sd_hbm,
    mixed_ref,
    load_ref,
    tok,
    normed,
    weights,
    stage,
    sg,
    su,
    sd,
    outgoing,
    arrived,
    result,
    returned,
    hidden,
    shidden,
    acc,
    csrc,
    cdst,
    local_sem,
    weight_sem,
    stage_sem,
    send_sem,
    recv_sem,
    back_send,
    back_recv,
    csend,
    crecv,
    ysend,
    yrecv,
    zsend,
    zrecv,
    ready,
):
    ep, tp = lax.axis_index("ep"), lax.axis_index("tp")
    my_y, my_x = tp // NX, tp % NX
    my_z, core = ep // 2, ep % 2

    def device(dy=0, dx=0, dz=0, on=None):
        return {
            "ep": lax.rem(my_z + dz + NZ, NZ) * 2 + (core if on is None else on),
            "tp": lax.rem(my_y + dy + NY, NY) * NX + lax.rem(my_x + dx + NX, NX),
        }

    def remote(src, dst, send, recv, to):
        return pltpu.make_async_remote_copy(
            src_ref=src, dst_ref=dst, send_sem=send, recv_sem=recv, device_id=to, device_id_type=MESH
        )

    def signal(sem, to):
        pl.semaphore_signal(sem, inc=1, device_id=to, device_id_type=MESH)

    barrier = pltpu.get_barrier_semaphore()
    peers = (
        [device(dy, dx) for dy in range(-2, 3) for dx in range(NX) if (dy, dx) != (0, 0)]
        + [device(dy=d) for d in (3, 4, 5)]
        + [device(dz=d) for d in range(1, NZ)]
    )
    for peer in peers:
        signal(barrier, peer)

    copies = [
        pltpu.make_async_copy(src, dst, local_sem.at[i])
        for i, (src, dst) in enumerate(
            [(tokens_hbm, tok), (sg_hbm, sg), (su_hbm, su), (sd_hbm, sd)]
        )
    ]
    copies[0].start()

    def block_of(k):
        at = pl.ds(k % 4 * 512, 512)
        return (wg_hbm.at[0, at, :], wu_hbm.at[0, at, :], wd_hbm.at[0, :, at])[k // 4]

    own = [
        pltpu.make_async_copy(block_of(k), weights.at[k], weight_sem.at[k]) for k in range(12)
    ]
    third = lax.rem(my_z, 4) * 512
    third = pl.multiple_of(third, 512)
    staged = [
        pltpu.make_async_copy(src, stage, stage_sem)
        for src in (
            wg_hbm.at[0, pl.ds(third, 512), :],
            wu_hbm.at[0, pl.ds(third, 512), :],
            wd_hbm.at[0, :, pl.ds(third, 512)],
        )
    ]

    def sub(ref, piece, q):
        return ref.at[piece, pl.ds(q * SUB, SUB), :]

    def across(q):
        return remote(
            stage.at[pl.ds(q * SUB, SUB), :],
            sub(weights, my_z, q),
            ysend.at[q],
            yrecv.at[q],
            device(dy=4),
        )

    def round_z(way, step, q):
        sign = 1 - 2 * way
        piece = lax.rem(my_z - sign * (step - 1) + NZ, NZ)
        return remote(
            sub(weights, piece, q),
            sub(weights, piece, q),
            zsend.at[way, step - 1, q],
            zrecv.at[way, step - 1, q],
            device(dz=sign),
        )

    def goes(way, step, q):
        return step < 6 or (step == 6 and (q < SUBS // 2) == (way == 0))

    @pl.when(core == 1)
    def _():
        for part in range(3):

            @pl.when(my_z // 4 == part)
            def _():
                staged[part].start()

        pl.semaphore_wait(barrier, len(peers))
        signal(barrier, device(on=0))
        staged[0].wait()
        for q in range(SUBS):
            across(q).start()

    @pl.when(core == 0)
    def _():
        for c in own:
            c.start()

    for c in copies[1:]:
        c.start()

    shape = (SLOTS, 128)
    slot = lax.broadcasted_iota(jnp.int32, shape, 0)
    to_b = slot >= TO_A
    index = jnp.where(to_b, slot - TO_A + FIRST_B * NX, slot)
    shift = jnp.zeros(shape, jnp.int32)
    for g, dy in enumerate(SHIFTS):
        shift = jnp.where(index // NX == g, dy + NY, shift)
    shift = jnp.where(to_b, shift + NY // 2, shift)
    expert = (my_y + shift) % NY * NX + (my_x + index % NX) % NX
    routes = [routes_ref[k : k + 1, :] for k in range(2)]
    hot = [(r == expert).astype(F32) for r in routes]
    ti = lax.broadcasted_iota(jnp.int32, (128, 128), 0)
    tj = lax.broadcasted_iota(jnp.int32, (128, 128), 1)
    earlier = jnp.dot(
        (hot[0] + hot[1]).astype(BF16),
        (ti < tj).astype(F32).astype(BF16),
        preferred_element_type=F32,
    )
    at = earlier + (CAP * slot).astype(F32)
    pos_row = [jnp.sum(h * at, axis=0, keepdims=True).astype(jnp.int32) for h in hot]
    pos = [jnp.sum(jnp.where(ti == tj, p, 0), axis=1, keepdims=True) for p in pos_row]
    weight = [
        jnp.sum(jnp.where(ti == tj, gates_ref[k : k + 1, :], 0.0), axis=1, keepdims=True)
        for k in range(2)
    ]
    route_col = [jnp.sum(jnp.where(ti == tj, r, 0), axis=1, keepdims=True) for r in routes]
    counts = jnp.sum(
        (route_col[0] == tj).astype(F32) + (route_col[1] == tj).astype(F32), axis=0, keepdims=True
    )
    csrc[0] = jnp.broadcast_to(counts, (8, 128))

    copies[0].wait()
    gain = gain_ref[...]

    def norm(i, carry):
        rows = pl.ds(pl.multiple_of(i * 16, 16), 16)
        values = tok[rows, :].astype(F32)
        values = values - jnp.mean(values, axis=-1, keepdims=True)
        spread = jnp.mean(values * values, axis=-1, keepdims=True)
        normed[rows, :] = (values * lax.rsqrt(spread + 1e-05) * gain).astype(BF16)
        return carry

    lax.fori_loop(0, 8, norm, 0)

    def build(b):
        rows = slice(b * 128, (b + 1) * 128)
        pick = (ti + b * 128 == pos_row[0]) | (ti + b * 128 == pos_row[1])
        pick = jnp.where(pick, 1.0, 0.0).astype(BF16)
        for n in range(4):
            cols = slice(n * 512, (n + 1) * 512)
            outgoing[rows, cols] = jnp.dot(
                pick, normed[:, cols], preferred_element_type=F32
            ).astype(BF16)

    def rows_of(j):
        return pl.ds(pl.multiple_of(j * CAP, CAP), CAP)

    def dispatch(host, g, dx):
        j = g * NX + dx + (SLOTS - TO_A) * host
        r = g * GROUP + 2 * dx + core
        return remote(
            outgoing.at[rows_of(j)],
            arrived.at[rows_of(r)],
            send_sem.at[j],
            recv_sem.at[r],
            device(SHIFTS[g], dx, on=host),
        )

    last = len(SHIFTS) - 1
    to_partner = dispatch(1 - core, last, 0)
    self_j = SELF_A + (SELF_B - SELF_A) * core
    self_r = last * GROUP + core

    def arrival(g, dx, c):
        r = g * GROUP + 2 * dx + c
        return remote(
            outgoing.at[rows_of(0)], arrived.at[rows_of(r)], send_sem.at[0], recv_sem.at[r], device(dy=1)
        )

    def give_back(g, dx, c):
        r = g * GROUP + 2 * dx + c
        j = g * NX + dx + (SLOTS - TO_A) * core
        return remote(
            result.at[rows_of(r)],
            returned.at[rows_of(j)],
            back_send.at[r],
            back_recv.at[j],
            device(-SHIFTS[g], -dx, on=c),
        )

    def got_back(j):
        return remote(
            result.at[rows_of(0)], returned.at[rows_of(j)], back_send.at[0], back_recv.at[j], device(dy=1)
        )

    stages = (
        [device(dx=d) for d in range(1, NX)],
        [device(dy=d) for d in range(1, NY)],
        [device(dz=d) for d in range(1, NZ)],
        [device(on=1 - core)],
    )
    starts = [sum(len(s) for s in stages[:i]) for i in range(len(stages))]

    def count_copy(stage_at, i):
        n = starts[stage_at] + i
        return remote(csrc.at[stage_at], cdst.at[n], csend.at[n], crecv.at[n], stages[stage_at][i])

    def count_send(stage_at):
        for i in range(len(stages[stage_at])):
            count_copy(stage_at, i).start()

    def count_sum(stage_at):
        total = csrc[stage_at]
        for i in range(len(stages[stage_at])):
            count_copy(stage_at, i).wait_recv()
            total = total + cdst[starts[stage_at] + i]
        return total

    def send_block(b):
        for j in range(b * 8, (b + 1) * 8):
            if j in (SELF_A, SELF_B):
                continue
            host = int(j >= TO_A)
            i = j - (SLOTS - TO_A) * host
            dispatch(host, i // NX, i % NX).start()

    build(0)

    @pl.when(core == 0)
    def _():
        pl.semaphore_wait(barrier, len(peers) + 1)
        signal(ready, device(on=1))

    @pl.when(core == 1)
    def _():
        pl.semaphore_wait(ready, 1)

    for b in range(SLOTS // 8):
        if b + 1 < SLOTS // 8:
            build(b + 1)
        send_block(b)
    arrived[rows_of(self_r), :] = outgoing[rows_of(self_j), :]
    to_partner.start()
    count_send(0)

    for c in copies[1:]:
        c.wait()
    gate = jnp.dot(normed[...], sg[...], preferred_element_type=F32)
    up = jnp.dot(normed[...], su[...], preferred_element_type=F32)
    shidden[...] = (gate / (1.0 + jnp.exp(-gate)) * up).astype(BF16)
    for n in range(4):
        cols = slice(n * 512, (n + 1) * 512)
        acc[:, cols] = jnp.dot(shidden[...], sd[:, cols], preferred_element_type=F32)

    csrc[1] = count_sum(0)
    count_send(1)

    def serve(g):
        rows = slice(g * ROWS, (g + 1) * ROWS)
        pairs = [(dx, c) for dx in range(NX) for c in range(2) if (g, dx) != (last, 0)]
        for dx, c in pairs:
            arrival(g, dx, c).wait_recv()
        if g == last:
            arrival(g, 0, 1 - core).wait_recv()
        for n in range(2):
            cols = slice(n * 256, (n + 1) * 256)
            gate = jnp.zeros((ROWS, 256), F32)
            up = jnp.zeros((ROWS, 256), F32)
            for k in range(4):
                x = arrived[rows, k * 512 : (k + 1) * 512]
                gate = gate + jnp.dot(x, weights[k, :, cols], preferred_element_type=F32)
                up = up + jnp.dot(x, weights[4 + k, :, cols], preferred_element_type=F32)
            hidden[:, cols] = (gate / (1.0 + jnp.exp(-gate)) * up).astype(BF16)
        for n in range(4):
            cols = slice(n * 512, (n + 1) * 512)
            result[rows, cols] = jnp.dot(
                hidden[...], weights[8 + n], preferred_element_type=F32
            ).astype(BF16)
        for dx, c in pairs:
            give_back(g, dx, c).start()
        if g == last:
            give_back(g, 0, 1 - core).start()
            returned[rows_of(self_j), :] = result[rows_of(self_r), :]

    @pl.when(core == 0)
    def _():
        for c in own:
            c.wait()
        for g in range(FIRST_B):
            serve(g)

    @pl.when(core == 1)
    def _():
        for q in range(SUBS):
            across(q).wait_recv()
            for way in range(2):
                round_z(way, 1, q).start()
        for step in range(1, 7):
            for q in range(SUBS):
                for way in range(2):
                    if goes(way, step, q):
                        round_z(way, step, q).wait_recv()
                        if goes(way, step + 1, q):
                            round_z(way, step + 1, q).start()

    csrc[2] = count_sum(1)
    count_send(2)
    for g in range(FIRST_B, len(SHIFTS)):
        serve(g)
    csrc[3] = count_sum(2)
    count_send(3)

    for b in range(SLOTS // 8):
        rows = slice(b * 128, (b + 1) * 128)
        pick = jnp.concatenate(
            [jnp.where(tj + b * 128 == p, 1.0, 0.0).astype(BF16) for p in pos], axis=0
        )
        for j in range(b * 8, (b + 1) * 8):
            if j not in (SELF_A, SELF_B):
                got_back(j).wait_recv()
            else:

                @pl.when(core == int(j == SELF_A))
                def _():
                    got_back(j).wait_recv()

        for n in range(4):
            cols = slice(n * 512, (n + 1) * 512)
            pair = jnp.dot(pick, returned[rows, cols], preferred_element_type=F32)
            total = acc[:, cols] + (weight[0] * pair[:128] + weight[1] * pair[128:])
            if b + 1 < SLOTS // 8:
                acc[:, cols] = total
            else:
                mixed_ref[:, cols] = total.astype(BF16)

    load_ref[...] = count_sum(3)[0:1, 0:32] * (32 / 196608)

    for j in range(SLOTS):
        if j not in (SELF_A, SELF_B):
            host = int(j >= TO_A)
            i = j - (SLOTS - TO_A) * host
            dispatch(host, i // NX, i % NX).wait_send()
    to_partner.wait_send()

    def sent_back(g):
        for dx in range(NX):
            for c in range(2):
                if (g, dx) != (last, 0):
                    give_back(g, dx, c).wait_send()
        if g == last:
            give_back(g, 0, 1 - core).wait_send()

    for g in range(FIRST_B, len(SHIFTS)):
        sent_back(g)

    @pl.when(core == 0)
    def _():
        for g in range(FIRST_B):
            sent_back(g)

    @pl.when(core == 1)
    def _():
        for q in range(SUBS):
            across(q).wait_send()
        for step in range(1, 7):
            for q in range(SUBS):
                for way in range(2):
                    if goes(way, step, q):
                        round_z(way, step, q).wait_send()

    for stage_at in range(4):
        for i in range(len(stages[stage_at])):
            count_copy(stage_at, i).wait_send()


def per_device(tokens, norm_gain, routes, gates, wg, wu, wd, sg, su, sd):
    vmem = pl.BlockSpec(memory_space=pltpu.VMEM)
    anywhere = pl.BlockSpec(memory_space=pl.ANY)
    dma = pltpu.SemaphoreType.DMA
    landed = len(SHIFTS) * GROUP
    ncount = NX - 1 + NY - 1 + NZ - 1 + 1
    mixed, load = pl.pallas_call(
        kernel,
        out_shape=(
            jax.ShapeDtypeStruct((128, 2048), BF16),
            jax.ShapeDtypeStruct((1, 32), F32),
        ),
        in_specs=[vmem] * 3 + [anywhere] * 7,
        out_specs=(vmem, vmem),
        scratch_shapes=[
            pltpu.VMEM((128, 2048), BF16),
            pltpu.VMEM((128, 2048), BF16),
            pltpu.VMEM((12, 512, 512), BF16),
            pltpu.VMEM((512, 512), BF16),
            pltpu.VMEM((2048, 256), BF16),
            pltpu.VMEM((2048, 256), BF16),
            pltpu.VMEM((256, 2048), BF16),
            pltpu.VMEM((SLOTS * CAP, 2048), BF16),
            pltpu.VMEM((landed * CAP, 2048), BF16),
            pltpu.VMEM((landed * CAP, 2048), BF16),
            pltpu.VMEM((SLOTS * CAP, 2048), BF16),
            pltpu.VMEM((ROWS, 512), BF16),
            pltpu.VMEM((128, 256), BF16),
            pltpu.VMEM((128, 2048), F32),
            pltpu.VMEM((4, 8, 128), F32),
            pltpu.VMEM((ncount, 8, 128), F32),
            dma((4,)),
            dma((12,)),
            dma(()),
            dma((SLOTS,)),
            dma((landed,)),
            dma((landed,)),
            dma((SLOTS,)),
            dma((ncount,)),
            dma((ncount,)),
            dma((SUBS,)),
            dma((SUBS,)),
            dma((2, 6, SUBS)),
            dma((2, 6, SUBS)),
            pltpu.SemaphoreType.REGULAR,
        ],
        compiler_params=pltpu.CompilerParams(
            collective_id=0, has_side_effects=True, vmem_limit_bytes=60 << 20
        ),
    )(routes.T, gates.T, norm_gain.reshape(1, -1), tokens, wg, wu, wd, sg, su, sd)
    return mixed, load.reshape(32)


def solution(mesh):
    rows = P(("ep", "tp"), None)
    expert = P("tp", None, None)
    return jax.shard_map(
        per_device,
        mesh=mesh,
        in_specs=(rows, P(), rows, rows, expert, expert, expert, P(), P(), P()),
        out_specs=(rows, P()),
        check_vma=False,
    )
```

```python
import functools

import jax
import jax.numpy as jnp
from jax import lax
from jax.experimental import pallas as pl
from jax.experimental.pallas import tpu as pltpu
from jax.sharding import PartitionSpec as P

NY, NX, NZ = 8, 4, 12
CAP = 16
MESH = pl.DeviceIdType.MESH
F32, BF16 = jnp.float32, jnp.bfloat16

SHIFTS = (0, -1, 1, -2, 2)
TO_B = 3
FIRST_B = len(SHIFTS) * NX
SLOTS = FIRST_B + TO_B * NX
OFFSETS = [(dy, dx) for dy in SHIFTS + SHIFTS[:TO_B] for dx in range(NX)]
BLOCKS = ((0, 4), (4, 12), (12, 20), (20, 24), (24, 32))
BACK = ((0, 4), (4, 12), (12, 20), (20, 32))
TOTAL = SLOTS * CAP
SUB = 64
PARTS = (4,4)
SUBS = max(PARTS)
SHARE = (PARTS[0] * SUB, PARTS[1] * SUB)
UP = (5, 5, 5, 5, 5, 5, 5, 5, 5, 6, 6, 6)


def kernel(
    routes_hbm,
    gates_hbm,
    gain_hbm,
    tokens_hbm,
    wg_hbm,
    wu_hbm,
    wd_hbm,
    sg_hbm,
    su_hbm,
    sd_hbm,
    mixed_ref,
    load_ref,
    routes_ref,
    gates_ref,
    gain_ref,
    tok,
    normed,
    weights_a,
    weights_b,
    stage,
    sg,
    su,
    sd,
    outgoing,
    arrived,
    result,
    returned,
    hidden,
    shidden,
    acc,
    csrc,
    cz,
    cplane,
    cpair,
    local_sem,
    own_sem,
    stage_sem,
    send_sem,
    recv_sem,
    back_send,
    back_recv,
    csend,
    crecv,
    ysend,
    yrecv,
    zsend,
    zrecv,
    psend,
    precv,
    zready,
    yready,
    all_z,
):
    ep, tp = lax.axis_index("ep"), lax.axis_index("tp")
    my_y, my_x = tp // NX, tp % NX
    my_z, core = ep // 2, ep % 2

    def device(dy=0, dx=0, dz=0):
        return {
            "ep": lax.rem(my_z + dz + NZ, NZ) * 2 + core,
            "tp": lax.rem(my_y + dy + NY, NY) * NX + lax.rem(my_x + dx + NX, NX),
        }

    partner = {"ep": my_z * 2 + 1 - core, "tp": tp}

    def remote(src, dst, send, recv, to):
        return pltpu.make_async_remote_copy(
            src_ref=src, dst_ref=dst, send_sem=send, recv_sem=recv, device_id=to, device_id_type=MESH
        )

    def signal(sem, to):
        pl.semaphore_signal(sem, inc=1, device_id=to, device_id_type=MESH)

    copies = [
        pltpu.make_async_copy(src, dst, local_sem.at[i])
        for i, (src, dst) in enumerate(
            [
                (tokens_hbm, tok),
                (routes_hbm, routes_ref),
                (gates_hbm, gates_ref),
                (gain_hbm, gain_ref),
                (sg_hbm, sg),
                (su_hbm, su),
                (sd_hbm, sd),
            ]
        )
    ]
    quarter = pl.multiple_of(lax.rem(my_z, 4) * 512, 512)
    def each_core(act):
        for c in range(2):

            @pl.when(core == c)
            def _():
                act(c)

    def begin(c):
        return c * SHARE[0]

    def staged(c, part):
        mine = pl.ds(pl.multiple_of(quarter + begin(c), SUB), SHARE[c])
        src = (
            wg_hbm.at[0, mine, :],
            wu_hbm.at[0, mine, :],
            wd_hbm.at[0, begin(c) : begin(c) + SHARE[c], pl.ds(quarter, 512)],
        )[part]
        return pltpu.make_async_copy(src, stage.at[0 : SHARE[c], :], stage_sem)

    for part in range(3):

        @pl.when(my_z // 4 == part)
        def _():
            each_core(lambda c: staged(c, part).start())

    for c in copies[:4]:
        c.start()

    own = [
        pltpu.make_async_copy(wg_hbm.at[0], weights_a.at[0:2048, :], own_sem.at[0]),
        pltpu.make_async_copy(wu_hbm.at[0], weights_a.at[2048:4096, :], own_sem.at[1]),
    ] + [
        pltpu.make_async_copy(
            wd_hbm.at[0, :, k * 512 : (k + 1) * 512],
            weights_a.at[(8 + k) * 512 : (9 + k) * 512, :],
            own_sem.at[2],
        )
        for k in range(4)
    ]
    own_down = pltpu.make_async_copy(wg_hbm.at[0], weights_a.at[4096:6144, :], own_sem.at[2])

    def sub(k, q):
        return weights_b.at[pl.ds(pl.multiple_of(k * 512 + core * SHARE[0] + q * SUB, SUB), SUB), :]

    def across(q):
        return remote(
            stage.at[pl.ds(q * SUB, SUB), :], sub(my_z, q), ysend, yrecv.at[q], device(dy=4)
        )

    def round_z(way, step, q):
        sign = 1 - 2 * way
        at = sub(lax.rem(my_z - sign * (step - 1) + NZ, NZ), q)
        return remote(at, at, zsend, zrecv.at[way, step - 1, q], device(dz=sign))

    def over(way, step, q):
        at = sub(lax.rem(my_z - (1 - 2 * way) * step + NZ, NZ), q)
        return remote(at, at, psend, precv, partner)


    barrier = pltpu.get_barrier_semaphore()
    near = [(dy, dx) for dy in SHIFTS for dx in range(NX) if (dy, dx) != (0, 0)]
    for dy, dx in near:
        signal(barrier, device(dy, dx))
    signal(barrier, partner)

    for d in range(1, NZ):

        @pl.when(my_z + d < NZ)
        def _():
            signal(barrier, device(dz=d))

    @pl.when(my_y < NY // 2)
    def _():
        signal(barrier, device(dy=4))

    for c in own + copies[4:]:
        c.start()

    for c in copies[1:4]:
        c.wait()

    shape = (SLOTS, 128)
    slot = lax.broadcasted_iota(jnp.int32, shape, 0)
    to_b = slot >= FIRST_B
    index = jnp.where(to_b, slot - FIRST_B, slot)
    shift = jnp.zeros(shape, jnp.int32)
    for g, dy in enumerate(SHIFTS):
        shift = jnp.where(index // NX == g, dy + NY, shift)
    shift = jnp.where(to_b, shift + NY // 2, shift)
    expert = (my_y + shift) % NY * NX + (my_x + index % NX) % NX
    routes = [routes_ref[k : k + 1, :] for k in range(2)]
    hot = [(r == expert).astype(F32) for r in routes]
    ti = lax.broadcasted_iota(jnp.int32, (128, 128), 0)
    tj = lax.broadcasted_iota(jnp.int32, (128, 128), 1)
    earlier = jnp.dot(
        (hot[0] + hot[1]).astype(BF16),
        (ti < tj).astype(F32).astype(BF16),
        preferred_element_type=F32,
    )
    at = earlier + (CAP * slot).astype(F32)
    pos_row = [jnp.sum(h * at, axis=0, keepdims=True).astype(jnp.int32) for h in hot]
    pos = [jnp.sum(jnp.where(ti == tj, p, 0), axis=1, keepdims=True) for p in pos_row]
    weight = [
        jnp.sum(jnp.where(ti == tj, gates_ref[k : k + 1, :], 0.0), axis=1, keepdims=True)
        for k in range(2)
    ]
    route_col = [jnp.sum(jnp.where(ti == tj, r, 0), axis=1, keepdims=True) for r in routes]
    counts = jnp.sum(
        (route_col[0] == tj).astype(F32) + (route_col[1] == tj).astype(F32), axis=0, keepdims=True
    )
    csrc[0] = jnp.broadcast_to(counts, (8, 128))

    def enter():
        pl.semaphore_wait(barrier, len(near) + 1 + my_z + (my_y >= NY // 2).astype(jnp.int32))

        @pl.when(my_z > 0)
        def _():
            signal(zready.at[0], device(dz=-1))

        @pl.when(my_z == NZ - 1)
        def _():
            signal(zready.at[1], device(dz=1))

        for d in range(1, NZ):

            @pl.when(my_z >= d)
            def _():
                signal(all_z, device(dz=-d))

    def has(q):
        return functools.reduce(jnp.logical_or, [core == c for c in range(2) if q < PARTS[c]])

    def send_across():
        each_core(lambda c: staged(c, 0).wait())
        for q in range(SUBS):

            @pl.when(has(q))
            def _():
                across(q).start()

    @pl.when(my_y >= NY // 2)
    def _():
        enter()
        signal(yready, device(dy=4))
        send_across()

    copies[0].wait()
    gain = gain_ref[...]

    def norm(i, carry):
        rows = pl.ds(pl.multiple_of(i * 16, 16), 16)
        values = tok[rows, :].astype(F32)
        values = values - jnp.mean(values, axis=-1, keepdims=True)
        spread = jnp.mean(values * values, axis=-1, keepdims=True)
        normed[rows, :] = (values * lax.rsqrt(spread + 1e-05) * gain).astype(BF16)
        return carry

    lax.fori_loop(0, 8, norm, 0)

    def build(b):
        rows = slice(b * 128, (b + 1) * 128)
        pick = (ti + b * 128 == pos_row[0]) | (ti + b * 128 == pos_row[1])
        pick = jnp.where(pick, 1.0, 0.0).astype(BF16)
        for n in range(4):
            cols = slice(n * 512, (n + 1) * 512)
            outgoing[rows, cols] = jnp.dot(
                pick, normed[:, cols], preferred_element_type=F32
            ).astype(BF16)

    def rows_of(j):
        return slice(j * CAP, (j + 1) * CAP)

    def block_in(blocks, j):
        return [a <= j < b for a, b in blocks].index(True)

    def dispatch(j):
        dy, dx = OFFSETS[j]
        return remote(
            outgoing.at[rows_of(j), :],
            arrived.at[rows_of(j), :],
            send_sem,
            recv_sem.at[block_in(BLOCKS, j)],
            device(dy, dx),
        )

    def give_back(j):
        dy, dx = OFFSETS[j]
        return remote(
            result.at[rows_of(j), :],
            returned.at[rows_of(j), :],
            back_send,
            back_recv.at[block_in(BACK, j)],
            device(-dy, -dx),
        )

    def away(a, b):
        return [j for j in range(a, b) if OFFSETS[j] != (0, 0)]

    def wait_recv(n, sem):
        some = arrived.at[0 : n * CAP, :]
        remote(some, some, send_sem, sem, device(dy=1)).wait_recv()

    def wait_send(n, sem):
        some = arrived.at[0 : n * CAP, :]
        remote(some, some, sem, recv_sem.at[0], device(dy=1)).wait_send()

    others = [(dy, dx) for dy in range(NY) for dx in range(NX) if (dy, dx) != (0, 0)]

    def count_plane(i):
        return remote(csrc.at[0], cplane.at[i], csend, crecv.at[0], device(*others[i]))

    def count_z(i):
        return remote(csrc.at[1], cz.at[i], csend, crecv.at[1], device(dz=i + 1))

    def count_over():
        return remote(csrc.at[2], cpair, csend, crecv.at[2], partner)

    def wait_counts(ref, n, stage_at):
        some = ref.at[0:n]
        remote(some, some, csend, crecv.at[stage_at], device(dz=1)).wait_recv()
        total = csrc[stage_at]
        for i in range(n):
            total = total + ref[i]
        csrc[stage_at + 1] = total

    build(0)
    arrived[rows_of(0), :] = outgoing[rows_of(0), :]
    build(1)
    build(2)
    arrived[rows_of(FIRST_B), :] = outgoing[rows_of(FIRST_B), :]

    @pl.when(my_y < NY // 2)
    def _():
        enter()
        pl.semaphore_wait(yready, 1)
        signal(yready, device(dy=4))
        send_across()

    for j in away(0, 24):
        dispatch(j).start()
    build(3)
    for j in away(24, 32):
        dispatch(j).start()

    for c in copies[4:]:
        c.wait()
    gate = jnp.dot(normed[...], sg[...], preferred_element_type=F32)
    up = jnp.dot(normed[...], su[...], preferred_element_type=F32)
    shidden[...] = (gate / (1.0 + jnp.exp(-gate)) * up).astype(BF16)
    for n in range(4):
        cols = slice(n * 512, (n + 1) * 512)
        acc[:, cols] = jnp.dot(shidden[...], sd[:, cols], preferred_element_type=F32)

    def arrivals(i):
        wait_recv(len(away(*BLOCKS[i])), recv_sem.at[i])

    def serve(first, end, weights):
        rows = slice(first * CAP, end * CAP)
        m = (end - first) * CAP
        for n in range(2):
            cols = slice(n * 256, (n + 1) * 256)
            gate = jnp.zeros((m, 256), F32)
            up = jnp.zeros((m, 256), F32)
            for k in range(4):
                x = arrived[rows, k * 512 : (k + 1) * 512]
                gate = gate + jnp.dot(
                    x, weights[k * 512 : (k + 1) * 512, cols], preferred_element_type=F32
                )
                up = up + jnp.dot(
                    x, weights[2048 + k * 512 : 2048 + (k + 1) * 512, cols], preferred_element_type=F32
                )
            hidden[0:m, cols] = (gate / (1.0 + jnp.exp(-gate)) * up).astype(BF16)
        for n in range(4):
            cols = slice(n * 512, (n + 1) * 512)
            result[rows, cols] = jnp.dot(
                hidden[0:m, :],
                weights[4096 + n * 512 : 4096 + (n + 1) * 512, :],
                preferred_element_type=F32,
            ).astype(BF16)
        for j in range(first, end):
            if OFFSETS[j] == (0, 0):
                returned[rows_of(j), :] = result[rows_of(j), :]
            else:
                give_back(j).start()

    def own_weights():
        for c in own[:2]:
            c.wait()
        own_down.wait()

    def from_y(q):
        @pl.when(has(q))
        def _():
            across(q).wait_recv()
            remote(sub(my_z, q), sub(my_z, q), psend, precv, partner).start()

        if q == 0:

            @pl.when(my_z < NZ - 1)
            def _():
                pl.semaphore_wait(zready.at[0], 1)

        @pl.when(has(q))
        def _():
            round_z(0, 1, q).start()

        @pl.when(jnp.logical_and(my_z > 0, has(q)))
        def _():
            round_z(1, 1, q).start()

        if q == 0:
            @pl.when(my_y >= NY // 2)
            def _():
                pl.semaphore_wait(yready, 1)

            for i in range(len(others)):
                count_plane(i).start()

    def first_down():
        @pl.when(my_z == 0)
        def _():
            pl.semaphore_wait(zready.at[1], 1)
            for q in range(SUBS):

                @pl.when(has(q))
                def _():
                    round_z(1, 1, q).start()

    def any_of(planes):
        hits = [my_z == z for z in range(NZ) if z in planes]
        if len(hits) > NZ // 2:
            return jnp.logical_not(any_of([z for z in range(NZ) if z not in planes]))
        return functools.reduce(jnp.logical_or, hits, my_z < 0)

    def pass_on(way, step, q, planes):
        goes_on = [
            z
            for z in planes
            if step < (UP[(z - step) % NZ] if way == 0 else NZ - 1 - UP[(z + step) % NZ])
        ]

        @pl.when(jnp.logical_and(any_of(planes), has(q)))
        def _():
            round_z(way, step, q).wait_recv()

            @pl.when(any_of(goes_on))
            def _():
                round_z(way, step + 1, q).start()

            over(way, step, q).start()

    def settle_plane():
        wait_counts(cplane, len(others), 0)

        @pl.when(my_z < NZ - 1)
        def _():
            pl.semaphore_wait(all_z, NZ - 1 - my_z)

        for i in range(NZ - 1):
            count_z(i).start()

    def serve_a(i):
        arrivals(i)
        serve(*BLOCKS[i], weights_a)

    due = [
        (12.0, functools.partial(serve_a, 0)),
        (31.0, functools.partial(serve_a, 1)),
        (39.0, functools.partial(serve_a, 2)),
        (44.0, settle_plane),
        (12.0 + 9.4, first_down),
    ]
    for q in range(SUBS):
        due.append((12.0 + 2.2 * q, functools.partial(from_y, q)))
        for step in range(1, NZ // 2 + 1):
            usual = 12.0 + 5.65 * (step - 1) + (2.2 - 0.39375000000000004 * min(step - 1, 2)) * q
            down = [z for z in range(NZ) if step <= NZ - 1 - UP[(z + step) % NZ]]
            due.append((usual + 5.0, functools.partial(pass_on, 1, step, q, [z for z in down if z > 0])))
            if 0 in down:
                due.append((usual + 9.5, functools.partial(pass_on, 1, step, q, [0])))
            up = [z for z in range(NZ) if step <= UP[(z - step) % NZ]]
            due.append((usual + 3.0, functools.partial(pass_on, 0, step, q, [z for z in up if z >= step])))
            for z in up:
                if z < step:
                    due.append((usual + 3.0 + max(0.0, 12.5 - 2.5 * z), functools.partial(pass_on, 0, step, q, [z])))
    own_weights()
    for _, act in sorted(due, key=lambda d: d[0]):
        act()

    arrivals(3)
    arrivals(4)
    def bytes_of(rows, c, n):
        return rows.at[0 : n * SHARE[c], :]

    def other_part(c):
        some = bytes_of(weights_b, 1 - c, 12)
        remote(some, some, psend, precv, partner).wait_recv()

    each_core(other_part)
    serve(FIRST_B, SLOTS, weights_b)

    for i, (first, end) in enumerate(BACK):
        rows = slice(first * CAP, end * CAP)
        m = (end - first) * CAP
        where = lax.broadcasted_iota(jnp.int32, (128, m), 1) + first * CAP
        pick = jnp.concatenate(
            [jnp.where(where == p, 1.0, 0.0).astype(BF16) for p in pos], axis=0
        )
        if i == len(BACK) - 1:
            wait_counts(cz, NZ - 1, 1)
            count_over().start()
        wait_recv(len(away(first, end)), back_recv.at[i])
        for n in range(4):
            cols = slice(n * 512, (n + 1) * 512)
            pair = jnp.dot(pick, returned[rows, cols], preferred_element_type=F32)
            total = acc[:, cols] + (weight[0] * pair[:128] + weight[1] * pair[128:])
            if i + 1 < len(BACK):
                acc[:, cols] = total
            else:
                mixed_ref[:, cols] = total.astype(BF16)

    count_over().wait_recv()

    load_ref[...] = (csrc[2, 0:1, 0:32] + cpair[0:1, 0:32]) * (32 / 196608)

    wait_send(len(away(0, SLOTS)), send_sem)
    wait_send(len(away(0, SLOTS)), back_send)
    def passed(z):
        ups = sum(step <= UP[(z + 1 - step) % NZ] for step in range(1, NZ))
        downs = sum(step <= NZ - 1 - UP[(z - 1 + step) % NZ] for step in range(1, NZ))
        return ups + downs

    def weights_left(c):
        some = bytes_of(stage, c, 1)
        remote(some, some, ysend, yrecv.at[0], device(dy=4)).wait_send()
        some = bytes_of(weights_b, c, 12)
        remote(some, some, psend, precv, partner).wait_send()
        for n in sorted({passed(z) for z in range(NZ)}):

            @pl.when(any_of([z for z in range(NZ) if passed(z) == n]))
            def _():
                some = bytes_of(weights_b, c, n)
                remote(some, some, zsend, zrecv.at[0, 0, 0], device(dz=1)).wait_send()

    each_core(weights_left)
    some = cplane.at[0 : 11 + len(others) + 1]
    remote(some, some, csend, crecv.at[0], device(dz=1)).wait_send()


def per_device(tokens, norm_gain, routes, gates, wg, wu, wd, sg, su, sd):
    vmem = pl.BlockSpec(memory_space=pltpu.VMEM)
    anywhere = pl.BlockSpec(memory_space=pl.ANY)
    dma = pltpu.SemaphoreType.DMA
    regular = pltpu.SemaphoreType.REGULAR
    mixed, load = pl.pallas_call(
        kernel,
        out_shape=(
            pltpu.VMEM((128, 2048), BF16),
            pltpu.VMEM((1, 32), F32),
        ),
        in_specs=[anywhere] * 10,
        out_specs=(vmem, vmem),
        scratch_shapes=[
            pltpu.VMEM((2, 128), jnp.int32),
            pltpu.VMEM((2, 128), F32),
            pltpu.VMEM((1, 2048), F32),
            pltpu.VMEM((128, 2048), BF16),
            pltpu.VMEM((128, 2048), BF16),
            pltpu.VMEM((12 * 512, 512), BF16),
            pltpu.VMEM((12 * 512, 512), BF16),
            pltpu.VMEM((max(SHARE), 512), BF16),
            pltpu.VMEM((2048, 256), BF16),
            pltpu.VMEM((2048, 256), BF16),
            pltpu.VMEM((256, 2048), BF16),
            pltpu.VMEM((TOTAL, 2048), BF16),
            pltpu.VMEM((TOTAL, 2048), BF16),
            pltpu.VMEM((TOTAL, 2048), BF16),
            pltpu.VMEM((TOTAL, 2048), BF16),
            pltpu.VMEM((192, 512), BF16),
            pltpu.VMEM((128, 256), BF16),
            pltpu.VMEM((128, 2048), F32),
            pltpu.VMEM((3, 8, 128), F32),
            pltpu.VMEM((NZ - 1, 8, 128), F32),
            pltpu.VMEM((48, 8, 128), F32),
            pltpu.VMEM((8, 128), F32),
            dma((7,)),
            dma((3,)),
            dma(()),
            dma(()),
            dma((len(BLOCKS),)),
            dma(()),
            dma((len(BACK),)),
            dma(()),
            dma((3,)),
            dma(()),
            dma((SUBS,)),
            dma(()),
            dma((2, 6, SUBS)),
            dma(()),
            dma(()),
            regular((2,)),
            regular,
            regular,
        ],
        compiler_params=pltpu.CompilerParams(
            collective_id=0, has_side_effects=True, vmem_limit_bytes=60 << 20
        ),
    )(routes.T, gates.T, norm_gain.reshape(1, -1), tokens, wg, wu, wd, sg, su, sd)
    return mixed, load.reshape(32)


def solution(mesh):
    rows = P(("ep", "tp"), None)
    expert = P("tp", None, None)
    return jax.shard_map(
        per_device,
        mesh=mesh,
        in_specs=(rows, P(), rows, rows, expert, expert, expert, P(), P(), P()),
        out_specs=(rows, P()),
        check_vma=False,
    )
```

```python
import functools

import jax
import jax.numpy as jnp
from jax import lax
from jax.experimental import pallas as pl
from jax.experimental.pallas import tpu as pltpu
from jax.sharding import PartitionSpec as P

NY, NX, NZ = 8, 4, 12
CAP = 16
MESH = pl.DeviceIdType.MESH
F32, BF16 = jnp.float32, jnp.bfloat16

TO_A = (0, -1, 1, -2, 2)
TO_B = (0, -1, 1)
FIRST_B = len(TO_A) * NX
SLOTS = FIRST_B + len(TO_B) * NX
OFFSETS = [(dy, dx) for dy in TO_A + TO_B for dx in range(NX)]
SELF_A, SELF_B = FIRST_B - NX * (len(TO_A) - TO_A.index(0)), FIRST_B + NX * TO_B.index(0)
BLOCKS = ((0, 4), (4, 12), (12, 20), (20, 32))
BACK = ((0, 4), (4, 12), (12, 20), (20, 32))
TOTAL = SLOTS * CAP
SUB = 64
PARTS = (4,4)
SUBS = max(PARTS)
SHARE = (PARTS[0] * SUB, PARTS[1] * SUB)
SLOW_TO = 10
UP = (5, 5, 5, 5, 5, 5, 5, 5, 5, 6, 6, 6)


def kernel(
    routes_hbm,
    gates_hbm,
    gain_hbm,
    tokens_hbm,
    wg_hbm,
    wu_hbm,
    wd_hbm,
    sg_hbm,
    su_hbm,
    sd_hbm,
    mixed_ref,
    load_ref,
    routes_ref,
    gates_ref,
    gain_ref,
    tok,
    normed,
    weights_a,
    weights_b,
    stage,
    sg,
    su,
    sd,
    outgoing,
    arrived,
    result,
    returned,
    hidden,
    shidden,
    acc,
    csrc,
    cz,
    cplane,
    cpair,
    local_sem,
    own_sem,
    stage_sem,
    send_sem,
    recv_sem,
    back_send,
    back_recv,
    csend,
    crecv,
    ysend,
    yrecv,
    zsend,
    zrecv,
    psend,
    precv,
    zready,
    yready,
    all_z,
):
    ep, tp = lax.axis_index("ep"), lax.axis_index("tp")
    my_y, my_x = tp // NX, tp % NX
    my_z, core = ep // 2, ep % 2

    def device(dy=0, dx=0, dz=0):
        return {
            "ep": lax.rem(my_z + dz + NZ, NZ) * 2 + core,
            "tp": lax.rem(my_y + dy + NY, NY) * NX + lax.rem(my_x + dx + NX, NX),
        }

    partner = {"ep": my_z * 2 + 1 - core, "tp": tp}

    def remote(src, dst, send, recv, to):
        return pltpu.make_async_remote_copy(
            src_ref=src, dst_ref=dst, send_sem=send, recv_sem=recv, device_id=to, device_id_type=MESH
        )

    def signal(sem, to):
        pl.semaphore_signal(sem, inc=1, device_id=to, device_id_type=MESH)

    copies = [
        pltpu.make_async_copy(src, dst, local_sem.at[i])
        for i, (src, dst) in enumerate(
            [
                (tokens_hbm, tok),
                (routes_hbm, routes_ref),
                (gates_hbm, gates_ref),
                (gain_hbm, gain_ref),
                (sg_hbm, sg),
                (su_hbm, su),
                (sd_hbm, sd),
            ]
        )
    ]
    quarter = pl.multiple_of(lax.rem(my_z, 4) * 512, 512)
    def each_core(act):
        for c in range(2):

            @pl.when(core == c)
            def _():
                act(c)

    def begin(c):
        return c * SHARE[0]

    def staged(c, part):
        mine = pl.ds(pl.multiple_of(quarter + begin(c), SUB), SHARE[c])
        src = (
            wg_hbm.at[0, mine, :],
            wu_hbm.at[0, mine, :],
            wd_hbm.at[0, begin(c) : begin(c) + SHARE[c], pl.ds(quarter, 512)],
        )[part]
        return pltpu.make_async_copy(src, stage.at[0 : SHARE[c], :], stage_sem)

    for part in range(3):

        @pl.when(my_z // 4 == part)
        def _():
            each_core(lambda c: staged(c, part).start())

    for c in copies[:4]:
        c.start()

    own = [
        pltpu.make_async_copy(wg_hbm.at[0], weights_a.at[0:2048, :], own_sem.at[0]),
        pltpu.make_async_copy(wu_hbm.at[0], weights_a.at[2048:4096, :], own_sem.at[1]),
    ] + [
        pltpu.make_async_copy(
            wd_hbm.at[0, :, k * 512 : (k + 1) * 512],
            weights_a.at[(8 + k) * 512 : (9 + k) * 512, :],
            own_sem.at[2],
        )
        for k in range(4)
    ]
    own_down = pltpu.make_async_copy(wg_hbm.at[0], weights_a.at[4096:6144, :], own_sem.at[2])

    def sub(k, q):
        return weights_b.at[pl.ds(pl.multiple_of(k * 512 + core * SHARE[0] + q * SUB, SUB), SUB), :]

    def across(q):
        return remote(
            stage.at[pl.ds(q * SUB, SUB), :], sub(my_z, q), ysend, yrecv.at[q], device(dy=4)
        )

    def round_z(way, step, q):
        sign = 1 - 2 * way
        at = sub(lax.rem(my_z - sign * (step - 1) + NZ, NZ), q)
        return remote(at, at, zsend, zrecv.at[way, step - 1, q], device(dz=sign))

    def over(way, step, q):
        at = sub(lax.rem(my_z - (1 - 2 * way) * step + NZ, NZ), q)
        return remote(at, at, psend, precv, partner)


    barrier = pltpu.get_barrier_semaphore()
    near = [(dy, dx) for dy in TO_A for dx in range(NX) if (dy, dx) != (0, 0)]
    for dy, dx in near:
        signal(barrier, device(dy, dx))
    signal(barrier, partner)

    first = jnp.logical_and(tp == 0, core == 0)
    slow = jnp.logical_and(first, my_z == 0)
    over_slow = jnp.logical_and(first, jnp.logical_and(my_z > 0, my_z < SLOW_TO))

    @pl.when(over_slow)
    def _():
        signal(barrier, {"ep": core, "tp": tp})

    for d in range(1, NZ):

        @pl.when(jnp.logical_and(my_z + d < NZ, jnp.logical_not(jnp.logical_and(slow, d < SLOW_TO))))
        def _():
            signal(barrier, device(dz=d))

    @pl.when(my_y < NY // 2)
    def _():
        signal(barrier, device(dy=4))

    for c in own + copies[4:]:
        c.start()

    for c in copies[1:4]:
        c.wait()

    shape = (SLOTS, 128)
    slot = lax.broadcasted_iota(jnp.int32, shape, 0)
    shift = jnp.zeros(shape, jnp.int32)
    for g, dy in enumerate(TO_A + tuple(dy + NY // 2 for dy in TO_B)):
        shift = jnp.where(slot // NX == g, dy + NY, shift)
    expert = (my_y + shift) % NY * NX + (my_x + slot % NX) % NX
    routes = [routes_ref[k : k + 1, :] for k in range(2)]
    hot = [(r == expert).astype(F32) for r in routes]
    ti = lax.broadcasted_iota(jnp.int32, (128, 128), 0)
    tj = lax.broadcasted_iota(jnp.int32, (128, 128), 1)
    earlier = jnp.dot(
        (hot[0] + hot[1]).astype(BF16),
        (ti < tj).astype(F32).astype(BF16),
        preferred_element_type=F32,
    )
    at = earlier + (CAP * slot).astype(F32)
    pos_row = [jnp.sum(h * at, axis=0, keepdims=True).astype(jnp.int32) for h in hot]
    pos = [jnp.sum(jnp.where(ti == tj, p, 0), axis=1, keepdims=True) for p in pos_row]
    weight = [
        jnp.sum(jnp.where(ti == tj, gates_ref[k : k + 1, :], 0.0), axis=1, keepdims=True)
        for k in range(2)
    ]
    route_col = [jnp.sum(jnp.where(ti == tj, r, 0), axis=1, keepdims=True) for r in routes]
    counts = jnp.sum(
        (route_col[0] == tj).astype(F32) + (route_col[1] == tj).astype(F32), axis=0, keepdims=True
    )
    csrc[0] = jnp.broadcast_to(counts, (8, 128))

    def enter():
        early = my_z + (my_y >= NY // 2).astype(jnp.int32)
        early = early + jnp.where(slow, SLOW_TO - 1, 0) - over_slow.astype(jnp.int32)
        pl.semaphore_wait(barrier, len(near) + 1 + early)

        @pl.when(slow)
        def _():
            signal(zready.at[1], device(dz=1))
            for d in range(1, SLOW_TO):
                signal(all_z, device(dz=d))

        @pl.when(jnp.logical_and(my_z > 0, jnp.logical_not(jnp.logical_and(over_slow, my_z == 1))))
        def _():
            signal(zready.at[0], device(dz=-1))

        @pl.when(my_z == NZ - 1)
        def _():
            signal(zready.at[1], device(dz=1))

        for d in range(1, NZ):

            @pl.when(jnp.logical_and(my_z >= d, jnp.logical_not(jnp.logical_and(over_slow, my_z == d))))
            def _():
                signal(all_z, device(dz=-d))

    def has(q):
        return functools.reduce(jnp.logical_or, [core == c for c in range(2) if q < PARTS[c]])

    def send_across():
        each_core(lambda c: staged(c, 0).wait())
        for q in range(SUBS):

            @pl.when(has(q))
            def _():
                across(q).start()

    @pl.when(my_y >= NY // 2)
    def _():
        enter()
        signal(yready, device(dy=4))
        send_across()

    copies[0].wait()
    gain = gain_ref[...]

    def norm(i, carry):
        rows = pl.ds(pl.multiple_of(i * 16, 16), 16)
        values = tok[rows, :].astype(F32)
        values = values - jnp.mean(values, axis=-1, keepdims=True)
        spread = jnp.mean(values * values, axis=-1, keepdims=True)
        normed[rows, :] = (values * lax.rsqrt(spread + 1e-05) * gain).astype(BF16)
        return carry

    lax.fori_loop(0, 8, norm, 0, unroll=2)

    def build(b):
        rows = slice(b * 128, (b + 1) * 128)
        pick = (ti + b * 128 == pos_row[0]) | (ti + b * 128 == pos_row[1])
        pick = jnp.where(pick, 1.0, 0.0).astype(BF16)
        for n in range(4):
            cols = slice(n * 512, (n + 1) * 512)
            outgoing[rows, cols] = jnp.dot(
                pick, normed[:, cols], preferred_element_type=F32
            ).astype(BF16)

    def rows_of(j):
        return slice(j * CAP, (j + 1) * CAP)

    def block_in(blocks, j):
        return [a <= j < b for a, b in blocks].index(True)

    def dispatch(j):
        dy, dx = OFFSETS[j]
        return remote(
            outgoing.at[rows_of(j), :],
            arrived.at[rows_of(j), :],
            send_sem,
            recv_sem.at[block_in(BLOCKS, j)],
            device(dy, dx),
        )

    def give_back(j):
        dy, dx = OFFSETS[j]
        return remote(
            result.at[rows_of(j), :],
            returned.at[rows_of(j), :],
            back_send,
            back_recv.at[block_in(BACK, j)],
            device(-dy, -dx),
        )

    def away(a, b):
        return [j for j in range(a, b) if OFFSETS[j] != (0, 0)]

    def wait_recv(n, sem):
        some = arrived.at[0 : n * CAP, :]
        remote(some, some, send_sem, sem, device(dy=1)).wait_recv()

    def wait_send(n, sem):
        some = arrived.at[0 : n * CAP, :]
        remote(some, some, sem, recv_sem.at[0], device(dy=1)).wait_send()

    others = [(dy, dx) for dy in range(NY) for dx in range(NX) if (dy, dx) != (0, 0)]

    def count_plane(i):
        return remote(csrc.at[0], cplane.at[i], csend, crecv.at[0], device(*others[i]))

    def count_z(i):
        return remote(csrc.at[1], cz.at[i], csend, crecv.at[1], device(dz=i + 1))

    def count_over():
        return remote(csrc.at[2], cpair, csend, crecv.at[2], partner)

    def wait_counts(ref, n, stage_at):
        some = ref.at[0:n]
        remote(some, some, csend, crecv.at[stage_at], device(dz=1)).wait_recv()
        total = csrc[stage_at]
        for i in range(n):
            total = total + ref[i]
        csrc[stage_at + 1] = total

    for b in (0, 2, 1, 3):
        build(b)
    for j in (SELF_A, SELF_B):
        arrived[rows_of(j), :] = outgoing[rows_of(j), :]

    @pl.when(my_y < NY // 2)
    def _():
        enter()

    own_row = [j for j in range(SLOTS) if OFFSETS[j][0] == 0]
    for j in own_row:
        if j not in (SELF_A, SELF_B):
            dispatch(j).start()

    @pl.when(my_y < NY // 2)
    def _():
        pl.semaphore_wait(yready, 1)
        signal(yready, device(dy=4))
        send_across()

    for j in range(FIRST_B):
        if j not in own_row:
            dispatch(j).start()

    for c in copies[4:]:
        c.wait()
    gate = jnp.dot(normed[...], sg[...], preferred_element_type=F32)
    up = jnp.dot(normed[...], su[...], preferred_element_type=F32)
    shidden[...] = (gate / (1.0 + jnp.exp(-gate)) * up).astype(BF16)
    for n in range(4):
        cols = slice(n * 512, (n + 1) * 512)
        acc[:, cols] = jnp.dot(shidden[...], sd[:, cols], preferred_element_type=F32)

    def arrivals(i):
        wait_recv(len(away(*BLOCKS[i])), recv_sem.at[i])

    def serve(first, end, weights):
        rows = slice(first * CAP, end * CAP)
        m = (end - first) * CAP
        for n in range(2):
            cols = slice(n * 256, (n + 1) * 256)
            gate = jnp.zeros((m, 256), F32)
            up = jnp.zeros((m, 256), F32)
            for k in range(4):
                x = arrived[rows, k * 512 : (k + 1) * 512]
                gate = gate + jnp.dot(
                    x, weights[k * 512 : (k + 1) * 512, cols], preferred_element_type=F32
                )
                up = up + jnp.dot(
                    x, weights[2048 + k * 512 : 2048 + (k + 1) * 512, cols], preferred_element_type=F32
                )
            hidden[0:m, cols] = (gate / (1.0 + jnp.exp(-gate)) * up).astype(BF16)
        for n in range(4):
            cols = slice(n * 512, (n + 1) * 512)
            result[rows, cols] = jnp.dot(
                hidden[0:m, :],
                weights[4096 + n * 512 : 4096 + (n + 1) * 512, :],
                preferred_element_type=F32,
            ).astype(BF16)
        for j in range(first, end):
            if OFFSETS[j] == (0, 0):
                returned[rows_of(j), :] = result[rows_of(j), :]
            else:
                give_back(j).start()

    def own_weights():
        for c in own[:2]:
            c.wait()
        own_down.wait()

    def from_y(q):
        @pl.when(has(q))
        def _():
            across(q).wait_recv()
            remote(sub(my_z, q), sub(my_z, q), psend, precv, partner).start()

        if q == 0:

            @pl.when(jnp.logical_and(my_z < NZ - 1, jnp.logical_not(slow)))
            def _():
                pl.semaphore_wait(zready.at[0], 1)

            @pl.when(jnp.logical_and(over_slow, my_z == 1))
            def _():
                pl.semaphore_wait(zready.at[1], 1)

        @pl.when(has(q))
        def _():
            round_z(0, 1, q).start()

        @pl.when(jnp.logical_and(my_z > 0, has(q)))
        def _():
            round_z(1, 1, q).start()

        if q == 0:
            @pl.when(my_y >= NY // 2)
            def _():
                pl.semaphore_wait(yready, 1)

            for i in range(len(others)):
                count_plane(i).start()

    def first_down():
        @pl.when(my_z == 0)
        def _():
            pl.semaphore_wait(zready.at[1], 1)
            for q in range(SUBS):

                @pl.when(has(q))
                def _():
                    round_z(1, 1, q).start()

    def any_of(planes):
        hits = [my_z == z for z in range(NZ) if z in planes]
        if len(hits) > NZ // 2:
            return jnp.logical_not(any_of([z for z in range(NZ) if z not in planes]))
        return functools.reduce(jnp.logical_or, hits, my_z < 0)

    def pass_on(way, step, q, planes):
        goes_on = [
            z
            for z in planes
            if step < (UP[(z - step) % NZ] if way == 0 else NZ - 1 - UP[(z + step) % NZ])
        ]

        @pl.when(jnp.logical_and(any_of(planes), has(q)))
        def _():
            round_z(way, step, q).wait_recv()

            @pl.when(any_of(goes_on))
            def _():
                round_z(way, step + 1, q).start()

            over(way, step, q).start()

    def settle_plane():
        wait_counts(cplane, len(others), 0)

        @pl.when(my_z < NZ - 1)
        def _():
            answers = NZ - 1 - my_z + over_slow.astype(jnp.int32) - jnp.where(slow, SLOW_TO - 1, 0)
            pl.semaphore_wait(all_z, answers)

        for i in range(NZ - 1):
            count_z(i).start()

    def serve_a(i):
        arrivals(i)
        serve(*BLOCKS[i], weights_a)

    def send_b():
        for j in range(FIRST_B, SLOTS):
            if j not in own_row:
                dispatch(j).start()

    due = [
        (12.5, send_b),
(12.0, functools.partial(serve_a, 0)),
        (31.0, functools.partial(serve_a, 1)),
        (39.0, functools.partial(serve_a, 2)),
        (44.0, settle_plane),
        (12.0 + 9.4, first_down),
    ]
    for q in range(SUBS):
        due.append((12.0 + 2.2 * q, functools.partial(from_y, q)))
        for step in range(1, NZ // 2 + 1):
            usual = 12.0 + 5.65 * (step - 1) + (2.2 - 0.39375000000000004 * min(step - 1, 2)) * q
            down = [z for z in range(NZ) if step <= NZ - 1 - UP[(z + step) % NZ]]
            due.append((usual + 5.0, functools.partial(pass_on, 1, step, q, [z for z in down if z > 0])))
            if 0 in down:
                due.append((usual + 9.5, functools.partial(pass_on, 1, step, q, [0])))
            up = [z for z in range(NZ) if step <= UP[(z - step) % NZ]]
            due.append((usual + 3.0, functools.partial(pass_on, 0, step, q, [z for z in up if z >= step])))
            for z in up:
                if z < step:
                    due.append((usual + 3.0 + max(0.0, 12.5 - 2.5 * z), functools.partial(pass_on, 0, step, q, [z])))
    own_weights()
    for _, act in sorted(due, key=lambda d: d[0]):
        act()

    arrivals(3)
    def bytes_of(rows, c, n):
        return rows.at[0 : n * SHARE[c], :]

    def other_part(c):
        some = bytes_of(weights_b, 1 - c, 12)
        remote(some, some, psend, precv, partner).wait_recv()

    each_core(other_part)
    serve(*BLOCKS[-1], weights_b)

    for i, (first, end) in enumerate(BACK):
        rows = slice(first * CAP, end * CAP)
        m = (end - first) * CAP
        where = lax.broadcasted_iota(jnp.int32, (128, m), 1) + first * CAP
        pick = jnp.concatenate(
            [jnp.where(where == p, 1.0, 0.0).astype(BF16) for p in pos], axis=0
        )
        if i == len(BACK) - 1:
            wait_counts(cz, NZ - 1, 1)
            count_over().start()
        wait_recv(len(away(first, end)), back_recv.at[i])
        for n in range(4):
            cols = slice(n * 512, (n + 1) * 512)
            pair = jnp.dot(pick, returned[rows, cols], preferred_element_type=F32)
            total = acc[:, cols] + (weight[0] * pair[:128] + weight[1] * pair[128:])
            if i + 1 < len(BACK):
                acc[:, cols] = total
            else:
                mixed_ref[:, cols] = total.astype(BF16)

    count_over().wait_recv()

    load_ref[...] = (csrc[2, 0:1, 0:32] + cpair[0:1, 0:32]) * (32 / 196608)

    wait_send(len(away(0, SLOTS)), send_sem)
    wait_send(len(away(0, SLOTS)), back_send)
    def passed(z):
        ups = sum(step <= UP[(z + 1 - step) % NZ] for step in range(1, NZ))
        downs = sum(step <= NZ - 1 - UP[(z - 1 + step) % NZ] for step in range(1, NZ))
        return ups + downs

    def weights_left(c):
        some = bytes_of(stage, c, 1)
        remote(some, some, ysend, yrecv.at[0], device(dy=4)).wait_send()
        some = bytes_of(weights_b, c, 12)
        remote(some, some, psend, precv, partner).wait_send()
        for n in sorted({passed(z) for z in range(NZ)}):

            @pl.when(any_of([z for z in range(NZ) if passed(z) == n]))
            def _():
                some = bytes_of(weights_b, c, n)
                remote(some, some, zsend, zrecv.at[0, 0, 0], device(dz=1)).wait_send()

    each_core(weights_left)
    some = cplane.at[0 : 11 + len(others) + 1]
    remote(some, some, csend, crecv.at[0], device(dz=1)).wait_send()


def per_device(tokens, norm_gain, routes, gates, wg, wu, wd, sg, su, sd):
    vmem = pl.BlockSpec(memory_space=pltpu.VMEM)
    anywhere = pl.BlockSpec(memory_space=pl.ANY)
    dma = pltpu.SemaphoreType.DMA
    regular = pltpu.SemaphoreType.REGULAR
    mixed, load = pl.pallas_call(
        kernel,
        out_shape=(
            pltpu.VMEM((128, 2048), BF16),
            pltpu.VMEM((1, 32), F32),
        ),
        in_specs=[anywhere] * 10,
        out_specs=(vmem, vmem),
        scratch_shapes=[
            pltpu.VMEM((2, 128), jnp.int32),
            pltpu.VMEM((2, 128), F32),
            pltpu.VMEM((1, 2048), F32),
            pltpu.VMEM((128, 2048), BF16),
            pltpu.VMEM((128, 2048), BF16),
            pltpu.VMEM((12 * 512, 512), BF16),
            pltpu.VMEM((12 * 512, 512), BF16),
            pltpu.VMEM((max(SHARE), 512), BF16),
            pltpu.VMEM((2048, 256), BF16),
            pltpu.VMEM((2048, 256), BF16),
            pltpu.VMEM((256, 2048), BF16),
            pltpu.VMEM((TOTAL, 2048), BF16),
            pltpu.VMEM((TOTAL, 2048), BF16),
            pltpu.VMEM((TOTAL, 2048), BF16),
            pltpu.VMEM((TOTAL, 2048), BF16),
            pltpu.VMEM((192, 512), BF16),
            pltpu.VMEM((128, 256), BF16),
            pltpu.VMEM((128, 2048), F32),
            pltpu.VMEM((3, 8, 128), F32),
            pltpu.VMEM((NZ - 1, 8, 128), F32),
            pltpu.VMEM((48, 8, 128), F32),
            pltpu.VMEM((8, 128), F32),
            dma((7,)),
            dma((3,)),
            dma(()),
            dma(()),
            dma((len(BLOCKS),)),
            dma(()),
            dma((len(BACK),)),
            dma(()),
            dma((3,)),
            dma(()),
            dma((SUBS,)),
            dma(()),
            dma((2, 6, SUBS)),
            dma(()),
            dma(()),
            regular((2,)),
            regular,
            regular,
        ],
        compiler_params=pltpu.CompilerParams(
            collective_id=0, has_side_effects=True, vmem_limit_bytes=60 << 20
        ),
    )(routes.T, gates.T, norm_gain.reshape(1, -1), tokens, wg, wu, wd, sg, su, sd)
    return mixed, load.reshape(32)


def solution(mesh):
    rows = P(("ep", "tp"), None)
    expert = P("tp", None, None)
    return jax.shard_map(
        per_device,
        mesh=mesh,
        in_specs=(rows, P(), rows, rows, expert, expert, expert, P(), P(), P()),
        out_specs=(rows, P()),
        check_vma=False,
    )
```

```python
import functools

import jax
import jax.numpy as jnp
from jax import lax
from jax.experimental import pallas as pl
from jax.experimental.pallas import tpu as pltpu
from jax.sharding import PartitionSpec as P

NY, NX, NZ = 8, 4, 12
CAP = 16
MESH = pl.DeviceIdType.MESH
F32, BF16 = jnp.float32, jnp.bfloat16

TO_A = (0, -1, 1, -2, 2)
TO_B = (0, -1, 1)
FIRST_B = len(TO_A) * NX
SLOTS = FIRST_B + len(TO_B) * NX
OFFSETS = [(dy, dx) for dy in TO_A + TO_B for dx in range(NX)]
SELF_A, SELF_B = FIRST_B - NX * (len(TO_A) - TO_A.index(0)), FIRST_B + NX * TO_B.index(0)
BLOCKS = ((0, 4), (4, 12), (12, 20), (20, 32))
BACK = ((0, 4), (4, 12), (12, 20), (20, 24), (24, 32))
TOTAL = SLOTS * CAP
SUB = 64
PARTS = (4,4)
SUBS = max(PARTS)
SHARE = (PARTS[0] * SUB, PARTS[1] * SUB)
SLOW_TO = 10
UP = (5, 5, 5, 5, 5, 5, 5, 5, 5, 6, 6, 6)


def kernel(
    routes_hbm,
    gates_hbm,
    gain_hbm,
    tokens_hbm,
    wg_hbm,
    wu_hbm,
    wd_hbm,
    sg_hbm,
    su_hbm,
    sd_hbm,
    mixed_ref,
    load_ref,
    routes_ref,
    gates_ref,
    gain_ref,
    tok,
    normed,
    weights_a,
    weights_b,
    stage,
    sg,
    su,
    sd,
    outgoing,
    arrived,
    result,
    returned,
    hidden,
    shidden,
    acc,
    csrc,
    cz,
    cplane,
    cpair,
    local_sem,
    own_sem,
    stage_sem,
    send_sem,
    recv_sem,
    back_send,
    back_recv,
    csend,
    crecv,
    ysend,
    yrecv,
    zsend,
    zrecv,
    psend,
    precv,
    zready,
    yready,
    all_z,
):
    ep, tp = lax.axis_index("ep"), lax.axis_index("tp")
    my_y, my_x = tp // NX, tp % NX
    my_z, core = ep // 2, ep % 2

    def device(dy=0, dx=0, dz=0):
        return {
            "ep": lax.rem(my_z + dz + NZ, NZ) * 2 + core,
            "tp": lax.rem(my_y + dy + NY, NY) * NX + lax.rem(my_x + dx + NX, NX),
        }

    partner = {"ep": my_z * 2 + 1 - core, "tp": tp}

    def remote(src, dst, send, recv, to):
        return pltpu.make_async_remote_copy(
            src_ref=src, dst_ref=dst, send_sem=send, recv_sem=recv, device_id=to, device_id_type=MESH
        )

    def signal(sem, to):
        pl.semaphore_signal(sem, inc=1, device_id=to, device_id_type=MESH)

    copies = [
        pltpu.make_async_copy(src, dst, local_sem.at[i])
        for i, (src, dst) in enumerate(
            [
                (tokens_hbm, tok),
                (routes_hbm, routes_ref),
                (gates_hbm, gates_ref),
                (gain_hbm, gain_ref),
                (sg_hbm, sg),
                (su_hbm, su),
                (sd_hbm, sd),
            ]
        )
    ]
    quarter = pl.multiple_of(lax.rem(my_z, 4) * 512, 512)
    def each_core(act):
        for c in range(2):

            @pl.when(core == c)
            def _():
                act(c)

    def begin(c):
        return c * SHARE[0]

    def staged(c, part):
        mine = pl.ds(pl.multiple_of(quarter + begin(c), SUB), SHARE[c])
        src = (
            wg_hbm.at[0, mine, :],
            wu_hbm.at[0, mine, :],
            wd_hbm.at[0, begin(c) : begin(c) + SHARE[c], pl.ds(quarter, 512)],
        )[part]
        return pltpu.make_async_copy(src, stage.at[0 : SHARE[c], :], stage_sem)

    for part in range(3):

        @pl.when(my_z // 4 == part)
        def _():
            each_core(lambda c: staged(c, part).start())

    for c in copies[:4]:
        c.start()

    own = [
        pltpu.make_async_copy(wg_hbm.at[0], weights_a.at[0:2048, :], own_sem.at[0]),
        pltpu.make_async_copy(wu_hbm.at[0], weights_a.at[2048:4096, :], own_sem.at[1]),
    ] + [
        pltpu.make_async_copy(
            wd_hbm.at[0, :, k * 512 : (k + 1) * 512],
            weights_a.at[(8 + k) * 512 : (9 + k) * 512, :],
            own_sem.at[2],
        )
        for k in range(4)
    ]
    own_down = pltpu.make_async_copy(wg_hbm.at[0], weights_a.at[4096:6144, :], own_sem.at[2])

    def sub(k, q):
        return weights_b.at[pl.ds(pl.multiple_of(k * 512 + core * SHARE[0] + q * SUB, SUB), SUB), :]

    def across(q):
        return remote(
            stage.at[pl.ds(q * SUB, SUB), :], sub(my_z, q), ysend, yrecv.at[q], device(dy=4)
        )

    def round_z(way, step, q):
        sign = 1 - 2 * way
        at = sub(lax.rem(my_z - sign * (step - 1) + NZ, NZ), q)
        return remote(at, at, zsend, zrecv.at[way, step - 1, q], device(dz=sign))

    def over(way, step, q):
        at = sub(lax.rem(my_z - (1 - 2 * way) * step + NZ, NZ), q)
        return remote(at, at, psend, precv, partner)


    barrier = pltpu.get_barrier_semaphore()
    near = [(dy, dx) for dy in TO_A for dx in range(NX) if (dy, dx) != (0, 0)]
    for dy, dx in near:
        signal(barrier, device(dy, dx))
    signal(barrier, partner)

    first = jnp.logical_and(tp == 0, core == 0)
    slow = jnp.logical_and(first, my_z == 0)
    over_slow = jnp.logical_and(first, jnp.logical_and(my_z > 0, my_z < SLOW_TO))

    @pl.when(over_slow)
    def _():
        signal(barrier, {"ep": core, "tp": tp})

    for d in range(1, NZ):

        @pl.when(jnp.logical_and(my_z + d < NZ, jnp.logical_not(jnp.logical_and(slow, d < SLOW_TO))))
        def _():
            signal(barrier, device(dz=d))

    @pl.when(my_y < NY // 2)
    def _():
        signal(barrier, device(dy=4))

    for c in own + copies[4:]:
        c.start()

    for c in copies[1:4]:
        c.wait()

    shape = (SLOTS, 128)
    slot = lax.broadcasted_iota(jnp.int32, shape, 0)
    shift = jnp.zeros(shape, jnp.int32)
    for g, dy in enumerate(TO_A + tuple(dy + NY // 2 for dy in TO_B)):
        shift = jnp.where(slot // NX == g, dy + NY, shift)
    expert = (my_y + shift) % NY * NX + (my_x + slot % NX) % NX
    routes = [routes_ref[k : k + 1, :] for k in range(2)]
    hot = [(r == expert).astype(F32) for r in routes]
    ti = lax.broadcasted_iota(jnp.int32, (128, 128), 0)
    tj = lax.broadcasted_iota(jnp.int32, (128, 128), 1)
    earlier = jnp.dot(
        (hot[0] + hot[1]).astype(BF16),
        (ti < tj).astype(F32).astype(BF16),
        preferred_element_type=F32,
    )
    at = earlier + (CAP * slot).astype(F32)
    pos_row = [jnp.sum(h * at, axis=0, keepdims=True).astype(jnp.int32) for h in hot]
    pos = [jnp.sum(jnp.where(ti == tj, p, 0), axis=1, keepdims=True) for p in pos_row]
    weight = [
        jnp.sum(jnp.where(ti == tj, gates_ref[k : k + 1, :], 0.0), axis=1, keepdims=True)
        for k in range(2)
    ]
    route_col = [jnp.sum(jnp.where(ti == tj, r, 0), axis=1, keepdims=True) for r in routes]
    counts = jnp.sum(
        (route_col[0] == tj).astype(F32) + (route_col[1] == tj).astype(F32), axis=0, keepdims=True
    )
    csrc[0] = jnp.broadcast_to(counts, (8, 128))

    def enter():
        early = my_z + (my_y >= NY // 2).astype(jnp.int32)
        early = early + jnp.where(slow, SLOW_TO - 1, 0) - over_slow.astype(jnp.int32)
        pl.semaphore_wait(barrier, len(near) + 1 + early)

        @pl.when(slow)
        def _():
            signal(zready.at[1], device(dz=1))
            for d in range(1, SLOW_TO):
                signal(all_z, device(dz=d))

        @pl.when(jnp.logical_and(my_z > 0, jnp.logical_not(jnp.logical_and(over_slow, my_z == 1))))
        def _():
            signal(zready.at[0], device(dz=-1))

        @pl.when(my_z == NZ - 1)
        def _():
            signal(zready.at[1], device(dz=1))

        for d in range(1, NZ):

            @pl.when(jnp.logical_and(my_z >= d, jnp.logical_not(jnp.logical_and(over_slow, my_z == d))))
            def _():
                signal(all_z, device(dz=-d))

    def has(q):
        return functools.reduce(jnp.logical_or, [core == c for c in range(2) if q < PARTS[c]])

    def send_across():
        each_core(lambda c: staged(c, 0).wait())
        for q in range(SUBS):

            @pl.when(has(q))
            def _():
                across(q).start()

    @pl.when(my_y >= NY // 2)
    def _():
        enter()
        signal(yready, device(dy=4))
        send_across()

    copies[0].wait()
    gain = gain_ref[...]

    def norm(i, carry):
        rows = pl.ds(pl.multiple_of(i * 16, 16), 16)
        values = tok[rows, :].astype(F32)
        values = values - jnp.mean(values, axis=-1, keepdims=True)
        spread = jnp.mean(values * values, axis=-1, keepdims=True)
        normed[rows, :] = (values * lax.rsqrt(spread + 1e-05) * gain).astype(BF16)
        return carry

    lax.fori_loop(0, 8, norm, 0, unroll=2)

    def build(b):
        rows = slice(b * 128, (b + 1) * 128)
        pick = (ti + b * 128 == pos_row[0]) | (ti + b * 128 == pos_row[1])
        pick = jnp.where(pick, 1.0, 0.0).astype(BF16)
        for n in range(4):
            cols = slice(n * 512, (n + 1) * 512)
            outgoing[rows, cols] = jnp.dot(
                pick, normed[:, cols], preferred_element_type=F32
            ).astype(BF16)

    def rows_of(j):
        return slice(j * CAP, (j + 1) * CAP)

    def block_in(blocks, j):
        return [a <= j < b for a, b in blocks].index(True)

    def dispatch(j):
        dy, dx = OFFSETS[j]
        return remote(
            outgoing.at[rows_of(j), :],
            arrived.at[rows_of(j), :],
            send_sem,
            recv_sem.at[block_in(BLOCKS, j)],
            device(dy, dx),
        )

    def give_back(j):
        dy, dx = OFFSETS[j]
        return remote(
            result.at[rows_of(j), :],
            returned.at[rows_of(j), :],
            back_send,
            back_recv.at[block_in(BACK, j)],
            device(-dy, -dx),
        )

    def away(a, b):
        return [j for j in range(a, b) if OFFSETS[j] != (0, 0)]

    def wait_recv(n, sem):
        some = arrived.at[0 : n * CAP, :]
        remote(some, some, send_sem, sem, device(dy=1)).wait_recv()

    def wait_send(n, sem):
        some = arrived.at[0 : n * CAP, :]
        remote(some, some, sem, recv_sem.at[0], device(dy=1)).wait_send()

    others = [(dy, dx) for dy in range(NY) for dx in range(NX) if (dy, dx) != (0, 0)]

    def count_plane(i):
        return remote(csrc.at[0], cplane.at[i], csend, crecv.at[0], device(*others[i]))

    def count_z(i):
        return remote(csrc.at[1], cz.at[i], csend, crecv.at[1], device(dz=i + 1))

    def count_over():
        return remote(csrc.at[2], cpair, csend, crecv.at[2], partner)

    def wait_counts(ref, n, stage_at):
        some = ref.at[0:n]
        remote(some, some, csend, crecv.at[stage_at], device(dz=1)).wait_recv()
        total = csrc[stage_at]
        for i in range(n):
            total = total + ref[i]
        csrc[stage_at + 1] = total

    for b in (0, 2, 1, 3):
        build(b)
    for j in (SELF_A, SELF_B):
        arrived[rows_of(j), :] = outgoing[rows_of(j), :]

    @pl.when(my_y < NY // 2)
    def _():
        enter()

    own_row = [j for j in range(FIRST_B) if OFFSETS[j][0] == 0]
    for j in own_row:
        if j not in (SELF_A, SELF_B):
            dispatch(j).start()

    @pl.when(my_y < NY // 2)
    def _():
        pl.semaphore_wait(yready, 1)
        signal(yready, device(dy=4))
        send_across()

    for j in range(FIRST_B):
        if j not in own_row:
            dispatch(j).start()

    for c in copies[4:]:
        c.wait()
    gate = jnp.dot(normed[...], sg[...], preferred_element_type=F32)
    up = jnp.dot(normed[...], su[...], preferred_element_type=F32)
    shidden[...] = (gate / (1.0 + jnp.exp(-gate)) * up).astype(BF16)
    for n in range(4):
        cols = slice(n * 512, (n + 1) * 512)
        acc[:, cols] = jnp.dot(shidden[...], sd[:, cols], preferred_element_type=F32)

    def arrivals(i):
        wait_recv(len(away(*BLOCKS[i])), recv_sem.at[i])

    def serve(first, end, weights):
        rows = slice(first * CAP, end * CAP)
        m = (end - first) * CAP
        for n in range(2):
            cols = slice(n * 256, (n + 1) * 256)
            gate = jnp.zeros((m, 256), F32)
            up = jnp.zeros((m, 256), F32)
            for k in range(4):
                x = arrived[rows, k * 512 : (k + 1) * 512]
                gate = gate + jnp.dot(
                    x, weights[k * 512 : (k + 1) * 512, cols], preferred_element_type=F32
                )
                up = up + jnp.dot(
                    x, weights[2048 + k * 512 : 2048 + (k + 1) * 512, cols], preferred_element_type=F32
                )
            hidden[0:m, cols] = (gate / (1.0 + jnp.exp(-gate)) * up).astype(BF16)
        for n in range(4):
            cols = slice(n * 512, (n + 1) * 512)
            result[rows, cols] = jnp.dot(
                hidden[0:m, :],
                weights[4096 + n * 512 : 4096 + (n + 1) * 512, :],
                preferred_element_type=F32,
            ).astype(BF16)
        for j in reversed(range(first, end)):
            if OFFSETS[j] == (0, 0):
                returned[rows_of(j), :] = result[rows_of(j), :]
            else:
                give_back(j).start()

    def own_weights():
        for c in own[:2]:
            c.wait()
        own_down.wait()

    def from_y(q):
        @pl.when(has(q))
        def _():
            across(q).wait_recv()
            remote(sub(my_z, q), sub(my_z, q), psend, precv, partner).start()

        if q == 0:

            @pl.when(jnp.logical_and(my_z < NZ - 1, jnp.logical_not(slow)))
            def _():
                pl.semaphore_wait(zready.at[0], 1)

            @pl.when(jnp.logical_and(over_slow, my_z == 1))
            def _():
                pl.semaphore_wait(zready.at[1], 1)

        @pl.when(has(q))
        def _():
            round_z(0, 1, q).start()

        @pl.when(jnp.logical_and(my_z > 0, has(q)))
        def _():
            round_z(1, 1, q).start()

        if q == 0:
            @pl.when(my_y >= NY // 2)
            def _():
                pl.semaphore_wait(yready, 1)

            for i in range(len(others)):
                count_plane(i).start()

    def first_down():
        @pl.when(my_z == 0)
        def _():
            pl.semaphore_wait(zready.at[1], 1)
            for q in range(SUBS):

                @pl.when(has(q))
                def _():
                    round_z(1, 1, q).start()

    def any_of(planes):
        hits = [my_z == z for z in range(NZ) if z in planes]
        if len(hits) > NZ // 2:
            return jnp.logical_not(any_of([z for z in range(NZ) if z not in planes]))
        return functools.reduce(jnp.logical_or, hits, my_z < 0)

    def pass_on(way, step, q, planes):
        goes_on = [
            z
            for z in planes
            if step < (UP[(z - step) % NZ] if way == 0 else NZ - 1 - UP[(z + step) % NZ])
        ]

        @pl.when(jnp.logical_and(any_of(planes), has(q)))
        def _():
            round_z(way, step, q).wait_recv()

            @pl.when(any_of(goes_on))
            def _():
                round_z(way, step + 1, q).start()

            over(way, step, q).start()

    def settle_plane():
        wait_counts(cplane, len(others), 0)

        @pl.when(my_z < NZ - 1)
        def _():
            answers = NZ - 1 - my_z + over_slow.astype(jnp.int32) - jnp.where(slow, SLOW_TO - 1, 0)
            pl.semaphore_wait(all_z, answers)

        for i in range(NZ - 1):
            count_z(i).start()

    def serve_a(i):
        arrivals(i)
        serve(*BLOCKS[i], weights_a)

    def send_b():
        for j in [*range(FIRST_B + NX, SLOTS), *range(FIRST_B + 1, FIRST_B + NX)]:
            if j != SELF_B:
                dispatch(j).start()

    due = [
        (12.5, send_b),
(12.0, functools.partial(serve_a, 0)),
        (31.0, functools.partial(serve_a, 1)),
        (39.0, functools.partial(serve_a, 2)),
        (44.0, settle_plane),
        (12.0 + 9.4, first_down),
    ]
    for q in range(SUBS):
        due.append((12.0 + 2.2 * q, functools.partial(from_y, q)))
        for step in range(1, NZ // 2 + 1):
            usual = 12.0 + 5.65 * (step - 1) + (2.2 - 0.39375000000000004 * min(step - 1, 2)) * q
            down = [z for z in range(NZ) if step <= NZ - 1 - UP[(z + step) % NZ]]
            due.append((usual + 5.0, functools.partial(pass_on, 1, step, q, [z for z in down if z > 0])))
            if 0 in down:
                due.append((usual + 9.5, functools.partial(pass_on, 1, step, q, [0])))
            up = [z for z in range(NZ) if step <= UP[(z - step) % NZ]]
            due.append((usual + 3.0, functools.partial(pass_on, 0, step, q, [z for z in up if z >= step])))
            for z in up:
                if z < step:
                    due.append((usual + 3.0 + max(0.0, 12.5 - 2.5 * z), functools.partial(pass_on, 0, step, q, [z])))
    own_weights()
    for _, act in sorted(due, key=lambda d: d[0]):
        act()

    arrivals(3)
    def bytes_of(rows, c, n):
        return rows.at[0 : n * SHARE[c], :]

    def other_part(c):
        some = bytes_of(weights_b, 1 - c, 12)
        remote(some, some, psend, precv, partner).wait_recv()

    each_core(other_part)
    serve(*BLOCKS[-1], weights_b)

    for i, (first, end) in enumerate(BACK):
        rows = slice(first * CAP, end * CAP)
        m = (end - first) * CAP
        where = lax.broadcasted_iota(jnp.int32, (128, m), 1) + first * CAP
        pick = jnp.concatenate(
            [jnp.where(where == p, 1.0, 0.0).astype(BF16) for p in pos], axis=0
        )
        if i == len(BACK) - 1:
            wait_counts(cz, NZ - 1, 1)
            count_over().start()
        wait_recv(len(away(first, end)), back_recv.at[i])
        for n in range(4):
            cols = slice(n * 512, (n + 1) * 512)
            pair = jnp.dot(pick, returned[rows, cols], preferred_element_type=F32)
            total = acc[:, cols] + (weight[0] * pair[:128] + weight[1] * pair[128:])
            if i + 1 < len(BACK):
                acc[:, cols] = total
            else:
                mixed_ref[:, cols] = total.astype(BF16)

    count_over().wait_recv()

    load_ref[...] = (csrc[2, 0:1, 0:32] + cpair[0:1, 0:32]) * (32 / 196608)

    wait_send(len(away(0, SLOTS)), send_sem)
    wait_send(len(away(0, SLOTS)), back_send)
    def passed(z):
        ups = sum(step <= UP[(z + 1 - step) % NZ] for step in range(1, NZ))
        downs = sum(step <= NZ - 1 - UP[(z - 1 + step) % NZ] for step in range(1, NZ))
        return ups + downs

    def weights_left(c):
        some = bytes_of(stage, c, 1)
        remote(some, some, ysend, yrecv.at[0], device(dy=4)).wait_send()
        some = bytes_of(weights_b, c, 12)
        remote(some, some, psend, precv, partner).wait_send()
        for n in sorted({passed(z) for z in range(NZ)}):

            @pl.when(any_of([z for z in range(NZ) if passed(z) == n]))
            def _():
                some = bytes_of(weights_b, c, n)
                remote(some, some, zsend, zrecv.at[0, 0, 0], device(dz=1)).wait_send()

    each_core(weights_left)
    some = cplane.at[0 : 11 + len(others) + 1]
    remote(some, some, csend, crecv.at[0], device(dz=1)).wait_send()


def per_device(tokens, norm_gain, routes, gates, wg, wu, wd, sg, su, sd):
    vmem = pl.BlockSpec(memory_space=pltpu.VMEM)
    anywhere = pl.BlockSpec(memory_space=pl.ANY)
    dma = pltpu.SemaphoreType.DMA
    regular = pltpu.SemaphoreType.REGULAR
    mixed, load = pl.pallas_call(
        kernel,
        out_shape=(
            pltpu.VMEM((128, 2048), BF16),
            pltpu.VMEM((1, 32), F32),
        ),
        in_specs=[anywhere] * 10,
        out_specs=(vmem, vmem),
        scratch_shapes=[
            pltpu.VMEM((2, 128), jnp.int32),
            pltpu.VMEM((2, 128), F32),
            pltpu.VMEM((1, 2048), F32),
            pltpu.VMEM((128, 2048), BF16),
            pltpu.VMEM((128, 2048), BF16),
            pltpu.VMEM((12 * 512, 512), BF16),
            pltpu.VMEM((12 * 512, 512), BF16),
            pltpu.VMEM((max(SHARE), 512), BF16),
            pltpu.VMEM((2048, 256), BF16),
            pltpu.VMEM((2048, 256), BF16),
            pltpu.VMEM((256, 2048), BF16),
            pltpu.VMEM((TOTAL, 2048), BF16),
            pltpu.VMEM((TOTAL, 2048), BF16),
            pltpu.VMEM((TOTAL, 2048), BF16),
            pltpu.VMEM((TOTAL, 2048), BF16),
            pltpu.VMEM((192, 512), BF16),
            pltpu.VMEM((128, 256), BF16),
            pltpu.VMEM((128, 2048), F32),
            pltpu.VMEM((3, 8, 128), F32),
            pltpu.VMEM((NZ - 1, 8, 128), F32),
            pltpu.VMEM((48, 8, 128), F32),
            pltpu.VMEM((8, 128), F32),
            dma((7,)),
            dma((3,)),
            dma(()),
            dma(()),
            dma((len(BLOCKS),)),
            dma(()),
            dma((len(BACK),)),
            dma(()),
            dma((3,)),
            dma(()),
            dma((SUBS,)),
            dma(()),
            dma((2, 6, SUBS)),
            dma(()),
            dma(()),
            regular((2,)),
            regular,
            regular,
        ],
        compiler_params=pltpu.CompilerParams(
            collective_id=0, has_side_effects=True, vmem_limit_bytes=60 << 20
        ),
    )(routes.T, gates.T, norm_gain.reshape(1, -1), tokens, wg, wu, wd, sg, su, sd)
    return mixed, load.reshape(32)


def solution(mesh):
    rows = P(("ep", "tp"), None)
    expert = P("tp", None, None)
    return jax.shard_map(
        per_device,
        mesh=mesh,
        in_specs=(rows, P(), rows, rows, expert, expert, expert, P(), P(), P()),
        out_specs=(rows, P()),
        check_vma=False,
    )
```

```python
import functools

import jax
import jax.numpy as jnp
from jax import lax
from jax.experimental import pallas as pl
from jax.experimental.pallas import tpu as pltpu
from jax.sharding import PartitionSpec as P

NY, NX, NZ = 8, 4, 12
CAP = 16
MESH = pl.DeviceIdType.MESH
F32, BF16 = jnp.float32, jnp.bfloat16

TO_A = (0, -1, 1, -2, 2)
TO_B = (0, -1, 1)
FIRST_B = len(TO_A) * NX
SLOTS = FIRST_B + len(TO_B) * NX
OFFSETS = [(dy, dx) for dy in TO_A + TO_B for dx in range(NX)]
SELF_A, SELF_B = FIRST_B - NX * (len(TO_A) - TO_A.index(0)), FIRST_B + NX * TO_B.index(0)
BLOCKS = ((0, 4), (4, 12), (12, 20), (20, 32))
BACK = ((0, 4), (4, 12), (12, 20), (20, 24), (24, 32))
TOTAL = SLOTS * CAP
SUB = 64
PARTS = (4,4)
SUBS = max(PARTS)
SHARE = (PARTS[0] * SUB, PARTS[1] * SUB)
SLOW_TO = 10
UP = (5, 5, 5, 5, 5, 5, 5, 5, 5, 6, 6, 6)


def kernel(
    routes_hbm,
    gates_hbm,
    gain_hbm,
    tokens_hbm,
    wg_hbm,
    wu_hbm,
    wd_hbm,
    sg_hbm,
    su_hbm,
    sd_hbm,
    mixed_ref,
    load_ref,
    routes_ref,
    gates_ref,
    gain_ref,
    tok,
    normed,
    weights_a,
    weights_b,
    stage,
    sg,
    su,
    sd,
    outgoing,
    arrived,
    result,
    returned,
    hidden,
    shidden,
    acc,
    csrc,
    cz,
    cplane,
    cpair,
    local_sem,
    own_sem,
    stage_sem,
    send_sem,
    recv_sem,
    back_send,
    back_recv,
    csend,
    crecv,
    ysend,
    yrecv,
    zsend,
    zrecv,
    psend,
    precv,
    zready,
    yready,
    all_z,
):
    ep, tp = lax.axis_index("ep"), lax.axis_index("tp")
    my_y, my_x = tp // NX, tp % NX
    my_z, core = ep // 2, ep % 2

    def device(dy=0, dx=0, dz=0):
        return {
            "ep": lax.rem(my_z + dz + NZ, NZ) * 2 + core,
            "tp": lax.rem(my_y + dy + NY, NY) * NX + lax.rem(my_x + dx + NX, NX),
        }

    partner = {"ep": my_z * 2 + 1 - core, "tp": tp}

    def remote(src, dst, send, recv, to):
        return pltpu.make_async_remote_copy(
            src_ref=src, dst_ref=dst, send_sem=send, recv_sem=recv, device_id=to, device_id_type=MESH
        )

    def signal(sem, to):
        pl.semaphore_signal(sem, inc=1, device_id=to, device_id_type=MESH)

    copies = [
        pltpu.make_async_copy(src, dst, local_sem.at[i])
        for i, (src, dst) in enumerate(
            [
                (tokens_hbm, tok),
                (routes_hbm, routes_ref),
                (gates_hbm, gates_ref),
                (gain_hbm, gain_ref),
                (sg_hbm, sg),
                (su_hbm, su),
                (sd_hbm, sd),
            ]
        )
    ]
    quarter = pl.multiple_of(lax.rem(my_z, 4) * 512, 512)
    def each_core(act):
        for c in range(2):

            @pl.when(core == c)
            def _():
                act(c)

    def begin(c):
        return c * SHARE[0]

    def staged(c, part):
        mine = pl.ds(pl.multiple_of(quarter + begin(c), SUB), SHARE[c])
        src = (
            wg_hbm.at[0, mine, :],
            wu_hbm.at[0, mine, :],
            wd_hbm.at[0, begin(c) : begin(c) + SHARE[c], pl.ds(quarter, 512)],
        )[part]
        return pltpu.make_async_copy(src, stage.at[0 : SHARE[c], :], stage_sem)

    for part in range(3):

        @pl.when(my_z // 4 == part)
        def _():
            each_core(lambda c: staged(c, part).start())

    for c in copies[:4]:
        c.start()

    own = [
        pltpu.make_async_copy(wg_hbm.at[0], weights_a.at[0:2048, :], own_sem.at[0]),
        pltpu.make_async_copy(wu_hbm.at[0], weights_a.at[2048:4096, :], own_sem.at[1]),
    ] + [
        pltpu.make_async_copy(
            wd_hbm.at[0, :, k * 512 : (k + 1) * 512],
            weights_a.at[(8 + k) * 512 : (9 + k) * 512, :],
            own_sem.at[2],
        )
        for k in range(4)
    ]
    own_down = pltpu.make_async_copy(wg_hbm.at[0], weights_a.at[4096:6144, :], own_sem.at[2])

    def sub(k, q):
        return weights_b.at[pl.ds(pl.multiple_of(k * 512 + core * SHARE[0] + q * SUB, SUB), SUB), :]

    def across(q):
        return remote(
            stage.at[pl.ds(q * SUB, SUB), :], sub(my_z, q), ysend, yrecv.at[q], device(dy=4)
        )

    def round_z(way, step, q):
        sign = 1 - 2 * way
        at = sub(lax.rem(my_z - sign * (step - 1) + NZ, NZ), q)
        return remote(at, at, zsend, zrecv.at[way, step - 1, q], device(dz=sign))

    def over(way, step, q):
        at = sub(lax.rem(my_z - (1 - 2 * way) * step + NZ, NZ), q)
        return remote(at, at, psend, precv, partner)


    barrier = pltpu.get_barrier_semaphore()
    near = [(dy, dx) for dy in TO_A for dx in range(NX) if (dy, dx) != (0, 0)]
    for dy, dx in near:
        signal(barrier, device(dy, dx))
    signal(barrier, partner)

    first = jnp.logical_and(tp == 0, core == 0)
    slow = jnp.logical_and(first, my_z == 0)
    over_slow = jnp.logical_and(first, jnp.logical_and(my_z > 0, my_z < SLOW_TO))

    @pl.when(over_slow)
    def _():
        signal(barrier, {"ep": core, "tp": tp})

    for d in range(1, NZ):

        @pl.when(jnp.logical_and(my_z + d < NZ, jnp.logical_not(jnp.logical_and(slow, d < SLOW_TO))))
        def _():
            signal(barrier, device(dz=d))

    @pl.when(my_y < NY // 2)
    def _():
        signal(barrier, device(dy=4))

    for c in own + copies[4:]:
        c.start()

    for c in copies[1:4]:
        c.wait()

    shape = (SLOTS, 128)
    slot = lax.broadcasted_iota(jnp.int32, shape, 0)
    shift = jnp.zeros(shape, jnp.int32)
    for g, dy in enumerate(TO_A + tuple(dy + NY // 2 for dy in TO_B)):
        shift = jnp.where(slot // NX == g, dy + NY, shift)
    expert = (my_y + shift) % NY * NX + (my_x + slot % NX) % NX
    routes = [routes_ref[k : k + 1, :] for k in range(2)]
    hot = [(r == expert).astype(F32) for r in routes]
    ti = lax.broadcasted_iota(jnp.int32, (128, 128), 0)
    tj = lax.broadcasted_iota(jnp.int32, (128, 128), 1)
    earlier = jnp.dot(
        (hot[0] + hot[1]).astype(BF16),
        (ti < tj).astype(F32).astype(BF16),
        preferred_element_type=F32,
    )
    at = earlier + (CAP * slot).astype(F32)
    pos_row = [jnp.sum(h * at, axis=0, keepdims=True).astype(jnp.int32) for h in hot]
    pos = [jnp.sum(jnp.where(ti == tj, p, 0), axis=1, keepdims=True) for p in pos_row]
    weight = [
        jnp.sum(jnp.where(ti == tj, gates_ref[k : k + 1, :], 0.0), axis=1, keepdims=True)
        for k in range(2)
    ]
    route_col = [jnp.sum(jnp.where(ti == tj, r, 0), axis=1, keepdims=True) for r in routes]
    counts = jnp.sum(
        (route_col[0] == tj).astype(F32) + (route_col[1] == tj).astype(F32), axis=0, keepdims=True
    )
    csrc[0] = jnp.broadcast_to(counts, (8, 128))

    def enter():
        early = my_z + (my_y >= NY // 2).astype(jnp.int32)
        early = early + jnp.where(slow, SLOW_TO - 1, 0) - over_slow.astype(jnp.int32)
        pl.semaphore_wait(barrier, len(near) + 1 + early)

        @pl.when(slow)
        def _():
            signal(zready.at[1], device(dz=1))
            for d in range(1, SLOW_TO):
                signal(all_z, device(dz=d))

        @pl.when(jnp.logical_and(my_z > 0, jnp.logical_not(jnp.logical_and(over_slow, my_z == 1))))
        def _():
            signal(zready.at[0], device(dz=-1))

        @pl.when(my_z == NZ - 1)
        def _():
            signal(zready.at[1], device(dz=1))

        for d in range(1, NZ):

            @pl.when(jnp.logical_and(my_z >= d, jnp.logical_not(jnp.logical_and(over_slow, my_z == d))))
            def _():
                signal(all_z, device(dz=-d))

    def has(q):
        return functools.reduce(jnp.logical_or, [core == c for c in range(2) if q < PARTS[c]])

    def send_across():
        each_core(lambda c: staged(c, 0).wait())
        for q in range(SUBS):

            @pl.when(has(q))
            def _():
                across(q).start()

    @pl.when(my_y >= NY // 2)
    def _():
        enter()
        signal(yready, device(dy=4))
        send_across()

    copies[0].wait()
    gain = gain_ref[...]

    def norm(i, carry):
        rows = pl.ds(pl.multiple_of(i * 16, 16), 16)
        values = tok[rows, :].astype(F32)
        values = values - jnp.mean(values, axis=-1, keepdims=True)
        spread = jnp.mean(values * values, axis=-1, keepdims=True)
        normed[rows, :] = (values * lax.rsqrt(spread + 1e-05) * gain).astype(BF16)
        return carry

    lax.fori_loop(0, 8, norm, 0, unroll=2)

    def build(b):
        rows = slice(b * 128, (b + 1) * 128)
        pick = (ti + b * 128 == pos_row[0]) | (ti + b * 128 == pos_row[1])
        pick = jnp.where(pick, 1.0, 0.0).astype(BF16)
        for n in range(4):
            cols = slice(n * 512, (n + 1) * 512)
            outgoing[rows, cols] = jnp.dot(
                pick, normed[:, cols], preferred_element_type=F32
            ).astype(BF16)

    def rows_of(j):
        return slice(j * CAP, (j + 1) * CAP)

    def block_in(blocks, j):
        return [a <= j < b for a, b in blocks].index(True)

    def dispatch(j):
        dy, dx = OFFSETS[j]
        return remote(
            outgoing.at[rows_of(j), :],
            arrived.at[rows_of(j), :],
            send_sem,
            recv_sem.at[block_in(BLOCKS, j)],
            device(dy, dx),
        )

    def give_back(j):
        dy, dx = OFFSETS[j]
        return remote(
            result.at[rows_of(j), :],
            returned.at[rows_of(j), :],
            back_send,
            back_recv.at[block_in(BACK, j)],
            device(-dy, -dx),
        )

    def away(a, b):
        return [j for j in range(a, b) if OFFSETS[j] != (0, 0)]

    def wait_recv(n, sem):
        some = arrived.at[0 : n * CAP, :]
        remote(some, some, send_sem, sem, device(dy=1)).wait_recv()

    def wait_send(n, sem):
        some = arrived.at[0 : n * CAP, :]
        remote(some, some, sem, recv_sem.at[0], device(dy=1)).wait_send()

    others = [(dy, dx) for dy in range(NY) for dx in range(NX) if (dy, dx) != (0, 0)]

    def count_plane(i):
        return remote(csrc.at[0], cplane.at[i], csend, crecv.at[0], device(*others[i]))

    def count_z(i):
        return remote(csrc.at[1], cz.at[i], csend, crecv.at[1], device(dz=i + 1))

    def count_over():
        return remote(csrc.at[2], cpair, csend, crecv.at[2], partner)

    def wait_counts(ref, n, stage_at):
        some = ref.at[0:n]
        remote(some, some, csend, crecv.at[stage_at], device(dz=1)).wait_recv()
        total = csrc[stage_at]
        for i in range(n):
            total = total + ref[i]
        csrc[stage_at + 1] = total

    for b in (0, 2, 1, 3):
        build(b)
    for j in (SELF_A, SELF_B):
        arrived[rows_of(j), :] = outgoing[rows_of(j), :]

    @pl.when(my_y < NY // 2)
    def _():
        enter()

    own_row = [j for j in range(FIRST_B) if OFFSETS[j][0] == 0]
    for j in own_row:
        if j not in (SELF_A, SELF_B):
            dispatch(j).start()

    @pl.when(my_y < NY // 2)
    def _():
        pl.semaphore_wait(yready, 1)
        signal(yready, device(dy=4))
        send_across()

    for j in [g * NX + dx for g in range(len(TO_A)) for dx in reversed(range(NX))]:
        if j not in own_row:
            dispatch(j).start()

    for c in copies[4:]:
        c.wait()
    gate = jnp.dot(normed[...], sg[...], preferred_element_type=F32)
    up = jnp.dot(normed[...], su[...], preferred_element_type=F32)
    shidden[...] = (gate / (1.0 + jnp.exp(-gate)) * up).astype(BF16)
    for n in range(4):
        cols = slice(n * 512, (n + 1) * 512)
        acc[:, cols] = jnp.dot(shidden[...], sd[:, cols], preferred_element_type=F32)

    def arrivals(i):
        wait_recv(len(away(*BLOCKS[i])), recv_sem.at[i])

    def serve(first, end, weights):
        rows = slice(first * CAP, end * CAP)
        m = (end - first) * CAP
        for n in range(2):
            cols = slice(n * 256, (n + 1) * 256)
            gate = jnp.zeros((m, 256), F32)
            up = jnp.zeros((m, 256), F32)
            for k in range(4):
                x = arrived[rows, k * 512 : (k + 1) * 512]
                gate = gate + jnp.dot(
                    x, weights[k * 512 : (k + 1) * 512, cols], preferred_element_type=F32
                )
                up = up + jnp.dot(
                    x, weights[2048 + k * 512 : 2048 + (k + 1) * 512, cols], preferred_element_type=F32
                )
            hidden[0:m, cols] = (gate / (1.0 + jnp.exp(-gate)) * up).astype(BF16)
        for n in range(4):
            cols = slice(n * 512, (n + 1) * 512)
            result[rows, cols] = jnp.dot(
                hidden[0:m, :],
                weights[4096 + n * 512 : 4096 + (n + 1) * 512, :],
                preferred_element_type=F32,
            ).astype(BF16)
        for j in reversed(range(first, end)):
            if OFFSETS[j] == (0, 0):
                returned[rows_of(j), :] = result[rows_of(j), :]
            else:
                give_back(j).start()

    def own_weights():
        for c in own[:2]:
            c.wait()
        own_down.wait()

    def from_y(q):
        @pl.when(has(q))
        def _():
            across(q).wait_recv()
            remote(sub(my_z, q), sub(my_z, q), psend, precv, partner).start()

        if q == 0:

            @pl.when(jnp.logical_and(my_z < NZ - 1, jnp.logical_not(slow)))
            def _():
                pl.semaphore_wait(zready.at[0], 1)

            @pl.when(jnp.logical_and(over_slow, my_z == 1))
            def _():
                pl.semaphore_wait(zready.at[1], 1)

        @pl.when(has(q))
        def _():
            round_z(0, 1, q).start()

        @pl.when(jnp.logical_and(my_z > 0, has(q)))
        def _():
            round_z(1, 1, q).start()

        if q == 0:
            @pl.when(my_y >= NY // 2)
            def _():
                pl.semaphore_wait(yready, 1)

            for i in range(len(others)):
                count_plane(i).start()

    def first_down():
        @pl.when(my_z == 0)
        def _():
            pl.semaphore_wait(zready.at[1], 1)
            for q in range(SUBS):

                @pl.when(has(q))
                def _():
                    round_z(1, 1, q).start()

    def any_of(planes):
        hits = [my_z == z for z in range(NZ) if z in planes]
        if len(hits) > NZ // 2:
            return jnp.logical_not(any_of([z for z in range(NZ) if z not in planes]))
        return functools.reduce(jnp.logical_or, hits, my_z < 0)

    def pass_on(way, step, q, planes):
        goes_on = [
            z
            for z in planes
            if step < (UP[(z - step) % NZ] if way == 0 else NZ - 1 - UP[(z + step) % NZ])
        ]

        @pl.when(jnp.logical_and(any_of(planes), has(q)))
        def _():
            round_z(way, step, q).wait_recv()

            @pl.when(any_of(goes_on))
            def _():
                round_z(way, step + 1, q).start()

            over(way, step, q).start()

    def settle_plane():
        wait_counts(cplane, len(others), 0)

        @pl.when(my_z < NZ - 1)
        def _():
            answers = NZ - 1 - my_z + over_slow.astype(jnp.int32) - jnp.where(slow, SLOW_TO - 1, 0)
            pl.semaphore_wait(all_z, answers)

        for i in range(NZ - 1):
            count_z(i).start()

    def serve_a(i):
        arrivals(i)
        serve(*BLOCKS[i], weights_a)

    def send_b():
        for j in [*range(FIRST_B + NX, SLOTS), *range(FIRST_B + 1, FIRST_B + NX)]:
            if j != SELF_B:
                dispatch(j).start()

    due = [
        (12.5, send_b),
(12.0, functools.partial(serve_a, 0)),
        (31.0, functools.partial(serve_a, 1)),
        (39.0, functools.partial(serve_a, 2)),
        (44.0, settle_plane),
        (12.0 + 9.4, first_down),
    ]
    for q in range(SUBS):
        due.append((12.0 + 2.2 * q, functools.partial(from_y, q)))
        for step in range(1, NZ // 2 + 1):
            usual = 12.0 + 5.65 * (step - 1) + (2.2 - 0.39375000000000004 * min(step - 1, 2)) * q
            down = [z for z in range(NZ) if step <= NZ - 1 - UP[(z + step) % NZ]]
            due.append((usual + 5.0, functools.partial(pass_on, 1, step, q, [z for z in down if z > 0])))
            if 0 in down:
                due.append((usual + 9.5, functools.partial(pass_on, 1, step, q, [0])))
            up = [z for z in range(NZ) if step <= UP[(z - step) % NZ]]
            due.append((usual + 3.0, functools.partial(pass_on, 0, step, q, [z for z in up if z >= step])))
            for z in up:
                if z < step:
                    due.append((usual + 3.0 + max(0.0, 12.5 - 2.5 * z), functools.partial(pass_on, 0, step, q, [z])))
    own_weights()
    for _, act in sorted(due, key=lambda d: d[0]):
        act()

    arrivals(3)
    def bytes_of(rows, c, n):
        return rows.at[0 : n * SHARE[c], :]

    def other_part(c):
        some = bytes_of(weights_b, 1 - c, 12)
        remote(some, some, psend, precv, partner).wait_recv()

    each_core(other_part)
    serve(*BLOCKS[-1], weights_b)

    for i, (first, end) in enumerate(BACK):
        rows = slice(first * CAP, end * CAP)
        m = (end - first) * CAP
        where = lax.broadcasted_iota(jnp.int32, (128, m), 1) + first * CAP
        pick = jnp.concatenate(
            [jnp.where(where == p, 1.0, 0.0).astype(BF16) for p in pos], axis=0
        )
        if i == len(BACK) - 1:
            wait_counts(cz, NZ - 1, 1)
            count_over().start()
        wait_recv(len(away(first, end)), back_recv.at[i])
        for n in range(4):
            cols = slice(n * 512, (n + 1) * 512)
            pair = jnp.dot(pick, returned[rows, cols], preferred_element_type=F32)
            total = acc[:, cols] + (weight[0] * pair[:128] + weight[1] * pair[128:])
            if i + 1 < len(BACK):
                acc[:, cols] = total
            else:
                mixed_ref[:, cols] = total.astype(BF16)

    count_over().wait_recv()

    load_ref[...] = (csrc[2, 0:1, 0:32] + cpair[0:1, 0:32]) * (32 / 196608)

    wait_send(len(away(0, SLOTS)), send_sem)
    wait_send(len(away(0, SLOTS)), back_send)
    def passed(z):
        ups = sum(step <= UP[(z + 1 - step) % NZ] for step in range(1, NZ))
        downs = sum(step <= NZ - 1 - UP[(z - 1 + step) % NZ] for step in range(1, NZ))
        return ups + downs

    def weights_left(c):
        some = bytes_of(stage, c, 1)
        remote(some, some, ysend, yrecv.at[0], device(dy=4)).wait_send()
        some = bytes_of(weights_b, c, 12)
        remote(some, some, psend, precv, partner).wait_send()
        for n in sorted({passed(z) for z in range(NZ)}):

            @pl.when(any_of([z for z in range(NZ) if passed(z) == n]))
            def _():
                some = bytes_of(weights_b, c, n)
                remote(some, some, zsend, zrecv.at[0, 0, 0], device(dz=1)).wait_send()

    each_core(weights_left)
    some = cplane.at[0 : 11 + len(others) + 1]
    remote(some, some, csend, crecv.at[0], device(dz=1)).wait_send()


def per_device(tokens, norm_gain, routes, gates, wg, wu, wd, sg, su, sd):
    vmem = pl.BlockSpec(memory_space=pltpu.VMEM)
    anywhere = pl.BlockSpec(memory_space=pl.ANY)
    dma = pltpu.SemaphoreType.DMA
    regular = pltpu.SemaphoreType.REGULAR
    mixed, load = pl.pallas_call(
        kernel,
        out_shape=(
            pltpu.VMEM((128, 2048), BF16),
            pltpu.VMEM((1, 32), F32),
        ),
        in_specs=[anywhere] * 10,
        out_specs=(vmem, vmem),
        scratch_shapes=[
            pltpu.VMEM((2, 128), jnp.int32),
            pltpu.VMEM((2, 128), F32),
            pltpu.VMEM((1, 2048), F32),
            pltpu.VMEM((128, 2048), BF16),
            pltpu.VMEM((128, 2048), BF16),
            pltpu.VMEM((12 * 512, 512), BF16),
            pltpu.VMEM((12 * 512, 512), BF16),
            pltpu.VMEM((max(SHARE), 512), BF16),
            pltpu.VMEM((2048, 256), BF16),
            pltpu.VMEM((2048, 256), BF16),
            pltpu.VMEM((256, 2048), BF16),
            pltpu.VMEM((TOTAL, 2048), BF16),
            pltpu.VMEM((TOTAL, 2048), BF16),
            pltpu.VMEM((TOTAL, 2048), BF16),
            pltpu.VMEM((TOTAL, 2048), BF16),
            pltpu.VMEM((192, 512), BF16),
            pltpu.VMEM((128, 256), BF16),
            pltpu.VMEM((128, 2048), F32),
            pltpu.VMEM((3, 8, 128), F32),
            pltpu.VMEM((NZ - 1, 8, 128), F32),
            pltpu.VMEM((48, 8, 128), F32),
            pltpu.VMEM((8, 128), F32),
            dma((7,)),
            dma((3,)),
            dma(()),
            dma(()),
            dma((len(BLOCKS),)),
            dma(()),
            dma((len(BACK),)),
            dma(()),
            dma((3,)),
            dma(()),
            dma((SUBS,)),
            dma(()),
            dma((2, 6, SUBS)),
            dma(()),
            dma(()),
            regular((2,)),
            regular,
            regular,
        ],
        compiler_params=pltpu.CompilerParams(
            collective_id=0, has_side_effects=True, vmem_limit_bytes=60 << 20
        ),
    )(routes.T, gates.T, norm_gain.reshape(1, -1), tokens, wg, wu, wd, sg, su, sd)
    return mixed, load.reshape(32)


def solution(mesh):
    rows = P(("ep", "tp"), None)
    expert = P("tp", None, None)
    return jax.shard_map(
        per_device,
        mesh=mesh,
        in_specs=(rows, P(), rows, rows, expert, expert, expert, P(), P(), P()),
        out_specs=(rows, P()),
        check_vma=False,
    )
```
